32 devices in a mesh: sp: 8 (over z, y), tp: 4 (over x, core).
Axes of the slice: x: 2, y: 2, z: 4, core: 2. Of those that a mesh axis runs over, the one named last changes fastest.
Arguments:
- target: bfloat16 [2048, 2048], P(('sp', 'tp')), may hold values from -6 to 6
- source: bfloat16 [4096, 2048], P(('sp', 'tp')), may hold values from -6 to 6
- target_gain: bfloat16 [2, 2048], replicated, may hold values from 0.099609375 to 1.8984375
- source_gain: bfloat16 [2, 2048], replicated, may hold values from 0.099609375 to 1.8984375
- query_w: bfloat16 [2, 2048, 8192], P(None, None, 'tp'), may hold values from -0.125 to 0.125
- key_w: bfloat16 [2, 2048, 4096], P(None, None, 'tp'), may hold values from -0.125 to 0.125
- value_w: bfloat16 [2, 2048, 4096], P(None, None, 'tp'), may hold values from -0.125 to 0.125
- out_w: bfloat16 [2, 8192, 2048], P(None, 'tp'), may hold values from -0.1875 to 0.1875
- head_temp: float32 [2, 16], P(None, 'tp'), may hold values from 1.5 to 8, as said below
- final_gain: bfloat16 [2048], replicated, may hold values from 0.099609375 to 1.8984375
Outputs:
- result: float32 [2048, 2048], P(('sp', 'tp'))
The draws below stay inside these ranges and needn't reach their ends.
Inputs may be any that keep to these rules, and one draw needn't show every extreme that they name: `head_temp`: a positive scale for each head's scores.
All inputs are finite; a program needn't handle non-finite values.
Results may differ from the reference program's by a relative error of at most 0.04.
Values may be sent and summed in bfloat16 or wider, within the bound.
A program may use at most 192 MiB of HBM per device.

```python
import math
import jax
import jax.numpy as jnp
from jax import lax

D = 2048
HEAD_DIM = 512
HEADS = 16
KV_HEADS = 8
SOURCE = 4096
TARGET = 2048
N_TP = 4


def draw_head_temp(key, part):
    moderate_key = jax.random.fold_in(key, 11)
    moderate = jnp.exp(jax.random.uniform(moderate_key, (2, HEADS), jnp.float32, math.log(1.5), math.log(3.5)))
    return moderate


def block_scale(stream_key, extent, cuts, smallest, high):
    level = 1.0
    for position, parts in cuts:
        draws = jax.random.uniform(jax.random.fold_in(jax.random.fold_in(stream_key, 6), position), (parts,), jnp.float32, smallest / len(cuts), high / len(cuts))
        level = level * jnp.repeat(jnp.exp(draws), extent[position] // parts).reshape((-1,) + (1,) * (len(extent) - 1 - position))
    return level


def noise(rng, extent, width, bound, cuts=(), kind=jnp.bfloat16):
    factor_of = block_scale(rng, extent, cuts, -0.22, 0.18) if cuts else 1.0
    array = jax.random.normal(rng, extent, jnp.float32) * width * factor_of
    return jnp.minimum(jnp.maximum(array, -bound), bound).astype(kind)


def setup_inputs(seed: int = 0) -> dict:
    splits = jax.random.split(jax.random.key(seed), 11)
    target = noise(splits[0], (TARGET, D), 1.0, 6.0, ((0, 32),))
    source = noise(splits[1], (SOURCE, D), 1.0, 6.0, ((0, 32),))
    target_gain = jnp.clip(1.0 + 0.18 * jax.random.normal(splits[2], (2, D), jnp.float32), 0.099609375, 1.8984375).astype(jnp.bfloat16)
    source_gain = jnp.clip(1.0 + 0.18 * jax.random.normal(splits[3], (2, D), jnp.float32), 0.099609375, 1.8984375).astype(jnp.bfloat16)
    query_w = noise(splits[4], (2, D, HEADS * HEAD_DIM), D ** -0.5, 0.125, ((2, 4),))
    key_w = noise(splits[5], (2, D, KV_HEADS * HEAD_DIM), D ** -0.5, 0.125, ((2, 4),))
    value_w = noise(splits[6], (2, D, KV_HEADS * HEAD_DIM), D ** -0.5, 0.125, ((2, 4),))
    out_w = noise(splits[7], (2, HEADS * HEAD_DIM, D), (3.0 * (HEADS * HEAD_DIM) ** -0.5), 0.1875, ((1, 4),))
    head_temp = draw_head_temp(jax.random.fold_in(splits[10], 71), 0)
    final_gain = jnp.clip(1.0 + 0.18 * jax.random.normal(splits[9], (D,), jnp.float32), 0.099609375, 1.8984375).astype(jnp.bfloat16)
    return dict(target=target, source=source, target_gain=target_gain, source_gain=source_gain, query_w=query_w, key_w=key_w, value_w=value_w, out_w=out_w, head_temp=head_temp, final_gain=final_gain)


EPS = 1e-06

def unit_rows(matrix):
    values = matrix.astype(jnp.float32)
    return values * lax.rsqrt(lax.optimization_barrier(jnp.mean(values * values, axis=-1, keepdims=True)) + EPS)

def attend_head(queries, key_rows, value_rows, scales):
    scores = jnp.dot(queries, key_rows.T, preferred_element_type=jnp.float32) * scales
    row_max = lax.optimization_barrier(jnp.max(scores, axis=-1, keepdims=True))
    exponent = jnp.exp(scores - row_max)
    row_total = lax.optimization_barrier(jnp.sum(exponent, axis=-1, keepdims=True))
    weights = exponent.astype(jnp.bfloat16)
    summed = jnp.dot(weights, value_rows, preferred_element_type=jnp.float32)
    return (summed / row_total).astype(jnp.bfloat16)

def reference(target, source, target_gain, source_gain, query_w, key_w, value_w, out_w, head_temp, final_gain):
    unit_source = unit_rows(source)
    group_size = HEADS // KV_HEADS
    head_share = HEADS // N_TP
    hidden_state = target.astype(jnp.float32)
    for layer_index in range(2):
        normed_source = (unit_source * source_gain[layer_index].astype(jnp.float32)).astype(jnp.bfloat16)
        key_rows = jnp.dot(normed_source, key_w[layer_index], preferred_element_type=jnp.float32).astype(jnp.bfloat16)
        value_rows = jnp.dot(normed_source, value_w[layer_index], preferred_element_type=jnp.float32).astype(jnp.bfloat16)
        key_rows = key_rows.reshape(SOURCE, KV_HEADS, HEAD_DIM)
        value_rows = value_rows.reshape(SOURCE, KV_HEADS, HEAD_DIM)
        normed = (unit_rows(hidden_state) * target_gain[layer_index].astype(jnp.float32)).astype(jnp.bfloat16)
        queries = jnp.dot(normed, query_w[layer_index], preferred_element_type=jnp.float32).astype(jnp.bfloat16)
        queries = queries.reshape(TARGET, HEADS, HEAD_DIM)
        scales = head_temp[layer_index].astype(jnp.float32) * HEAD_DIM ** (-0.5)

        def one_head(head_index):
            shared_head = head_index // group_size
            return attend_head(queries[:, head_index], key_rows[:, shared_head], value_rows[:, shared_head], scales[head_index])
        heads_out = lax.map(one_head, jnp.arange(HEADS, dtype=jnp.int32))
        heads_out = heads_out.reshape(N_TP, head_share, TARGET, HEAD_DIM)
        out_parts = out_w[layer_index].reshape(N_TP, head_share, HEAD_DIM, D)

        def part_term(running, inputs):
            head_block, weights = inputs
            partial_value = jnp.einsum('htd,hde->te', head_block.astype(jnp.float32), weights.astype(jnp.float32))
            rounded = lax.optimization_barrier(partial_value.astype(jnp.bfloat16))
            return (running + rounded.astype(jnp.float32), None)
        mixed, unused = lax.scan(part_term, jnp.zeros((TARGET, D), jnp.float32), (heads_out, out_parts))
        hidden_state = hidden_state + mixed
    return unit_rows(hidden_state) * final_gain.astype(jnp.float32)
```

```python
import functools
import math

import jax
import jax.numpy as jnp
from jax import lax
from jax.experimental import pallas as pl
from jax.experimental.pallas import tpu as pltpu
from jax.sharding import PartitionSpec as P

HEAD_DIM = 512
EPS = 1e-06
FLOOR = -1e30
CHUNK = 512
ROWS = 512
LOG2E = math.log2(math.e)
MESH = pl.DeviceIdType.MESH
MIB = 1024 * 1024
HBM = pl.BlockSpec(memory_space=pl.ANY)
VMEM = pl.BlockSpec(memory_space=pltpu.VMEM)
SMEM = pl.BlockSpec(memory_space=pltpu.SMEM)


def unit_rows(matrix):
    values = matrix.astype(jnp.float32)
    return values * lax.rsqrt(jnp.mean(values * values, axis=-1, keepdims=True) + EPS)


class Place:
    def __init__(self):
        sp, tp = lax.axis_index("sp"), lax.axis_index("tp")
        self.z, self.y = sp // 2, sp % 2
        self.x, self.core = tp // 2, tp % 2
        self.up, self.down = (self.z + 1) % 4, (self.z + 3) % 4
        self.far = (self.z + 2) % 4
        self.ox, self.oy, self.other = 1 - self.x, 1 - self.y, 1 - self.core

    def at(self, z=None, y=None, x=None, core=None):
        z = self.z if z is None else z
        y = self.y if y is None else y
        x = self.x if x is None else x
        core = self.core if core is None else core
        return (z * 2 + y, x * 2 + core)


class Copies:
    def __init__(self, send_sems, recv_sems):
        self.send_sems, self.recv_sems = send_sems, recv_sems
        self.index, self.sent = {}, []

    def _make(self, name, ref, target, dst=None):
        k = self.index.setdefault(name, len(self.index))
        return pltpu.make_async_remote_copy(
            src_ref=ref,
            dst_ref=ref if dst is None else dst,
            send_sem=self.send_sems.at[k],
            recv_sem=self.recv_sems.at[k],
            device_id=target,
            device_id_type=MESH,
        )

    def start(self, name, src, target, dst=None):
        self._make(name, src(), target, dst and dst()).start()
        self.sent.append((name, src, target, dst))

    def arrived(self, name, ref, source):
        self._make(name, ref, source).wait_recv()

    def drain(self):
        for name, src, target, dst in self.sent:
            self._make(name, src(), target, dst and dst()).wait_send()


def greet(targets):
    barrier = pltpu.get_barrier_semaphore()
    for target in targets:
        pl.semaphore_signal(barrier, inc=1, device_id=target, device_id_type=MESH)
    pl.semaphore_wait(barrier, len(targets))


def gather_kernel(
    own_ref, rows_ref, key_ref, value_ref, gain_ref,
    kv_ref, normed_ref,
    blocks, normed, weights, stage, send_sems, recv_sems, local_sems, weight_sems, out_sems,
):
    me = Place()
    z, y, x, core = me.z, me.y, me.x, me.core
    side = weights.shape[1] // 4
    steps = blocks.shape[0]

    def plane(c, zz):
        return blocks.at[c * 4 + zz]

    def column(c, yy, xx):
        return blocks.at[8 + c * 4 + yy * 2 + xx]

    loads = []
    for c in range(2):
        loads.append((own_ref.at[c], plane(c, z).at[y, x, core]))
        loads.append((own_ref.at[2 + c], column(c, y, x).at[z // 2, z % 2, core]))
        loads.append((rows_ref.at[c], normed.at[c, y, x, core]))
    loads = [
        pltpu.make_async_copy(src, dst, local_sems.at[k]) for k, (src, dst) in enumerate(loads)
    ]
    for copy in loads:
        copy.start()
    fetches = []
    for layer in range(2):
        for part, ref in enumerate((key_ref, value_ref)):
            n = 2 * layer + part
            fetches.append(
                pltpu.make_async_copy(
                    ref.at[layer, :, pl.ds(pl.multiple_of(y * side, side), side)],
                    weights.at[:, pl.ds(n * side, side)],
                    weight_sems.at[n],
                )
            )
    for copy in fetches:
        copy.start()
    greet([me.at(x=me.ox), me.at(y=me.oy), me.at(z=me.up), me.at(z=me.down), me.at(core=me.other)])
    for copy in loads:
        copy.wait()

    net = Copies(send_sems, recv_sems)
    sibling, xmate, ymate = me.at(core=me.other), me.at(x=me.ox), me.at(y=me.oy)
    above, below = me.at(z=me.up), me.at(z=me.down)

    def share(name, mine):
        net.start(name + "d", lambda: mine(core), sibling)

    def shared(name, mine):
        net.arrived(name + "d", mine(me.other), sibling)

    a_own = [lambda k, c=c: plane(c, z).at[y, x, k] for c in range(2)]
    a_one = [lambda k: plane(0, z).at[y, me.ox, k], lambda k: plane(1, z).at[me.oy, x, k]]
    a_two = [lambda k: plane(0, z).at[me.oy, :, k], lambda k: plane(1, z).at[:, me.ox, k]]
    a_have = [lambda k: plane(0, z).at[y, :, k], lambda k: plane(1, z).at[:, x, k]]
    a_all = [lambda k, c=c: plane(c, z).at[:, :, k] for c in range(2)]
    a_down = [lambda k, c=c: plane(c, me.down).at[:, :, k] for c in range(2)]
    a_up = [lambda k, c=c: plane(c, me.up).at[:, :, k] for c in range(2)]
    a_far = [lambda k, c=c: plane(c, me.far).at[:, :, k] for c in range(2)]
    b_own = [lambda k, c=c: column(c, y, x).at[z // 2, z % 2, k] for c in range(2)]
    b_down = [lambda k, c=c: column(c, y, x).at[me.down // 2, me.down % 2, k] for c in range(2)]
    b_up = [lambda k, c=c: column(c, y, x).at[me.up // 2, me.up % 2, k] for c in range(2)]
    b_far = [lambda k, c=c: column(c, y, x).at[me.far // 2, me.far % 2, k] for c in range(2)]
    b_all = [lambda k, c=c: column(c, y, x).at[:, :, k] for c in range(2)]
    b_one = [lambda k: column(0, me.oy, x).at[:, :, k], lambda k: column(1, y, me.ox).at[:, :, k]]
    b_two = [lambda k: column(0, y, me.ox).at[:, :, k], lambda k: column(1, me.oy, x).at[:, :, k]]
    b_last = [lambda k, c=c: column(c, me.oy, me.ox).at[:, :, k] for c in range(2)]
    t_own = [lambda k, c=c: normed.at[c, y, x, k] for c in range(2)]
    t_one = [lambda k: normed.at[0, y, me.ox, k], lambda k: normed.at[1, me.oy, x, k]]
    t_two = [lambda k: normed.at[0, me.oy, :, k], lambda k: normed.at[1, :, me.ox, k]]
    t_have = [lambda k: normed.at[0, y, :, k], lambda k: normed.at[1, :, x, k]]
    first = [xmate, ymate]
    second = [ymate, xmate]

    for c in range(2):
        net.start(f"a{c}1", lambda f=a_own[c]: f(core), first[c])
    for c in range(2):
        net.start(f"b{c}u", lambda f=b_own[c]: f(core), above)
        net.start(f"b{c}w", lambda f=b_own[c]: f(core), below)
    for c in range(2):
        net.start(f"t{c}1", lambda f=t_own[c]: f(core), first[c])
        share(f"b{c}0", b_own[c])
        share(f"a{c}0", a_own[c])
        share(f"t{c}0", t_own[c])

    def scale(n):
        fetches[n].wait()
        columns = pl.ds(n * side, side)

        def body(i, carry):
            block = pl.ds(i * 256, 256)
            weights[block, columns] = (
                weights[block, columns].astype(jnp.float32) * gain_ref[n // 2, block, :]
            ).astype(jnp.bfloat16)
            return carry

        lax.fori_loop(0, weights.shape[0] // 256, body, 0)

    scale(0)
    for c in range(2):
        net.arrived(f"a{c}1", a_one[c](core), first[c])
        net.start(f"a{c}2", lambda f=a_have[c]: f(core), second[c])
        share(f"a{c}1", a_one[c])
    scale(1)
    for c in range(2):
        net.arrived(f"b{c}u", b_down[c](core), below)
        if c == 0:
            net.start(f"b{c}f", lambda f=b_down[c]: f(core), above)
        share(f"b{c}1", b_down[c])
        net.arrived(f"b{c}w", b_up[c](core), above)
        if c == 1:
            net.start(f"b{c}f", lambda f=b_up[c]: f(core), below)
        share(f"b{c}2", b_up[c])
    for c in range(2):
        net.arrived(f"t{c}1", t_one[c](core), first[c])
        net.start(f"t{c}2", lambda f=t_have[c]: f(core), second[c])
        share(f"t{c}1", t_one[c])
    scale(2)
    for c in range(2):
        net.arrived(f"b{c}f", b_far[c](core), below if c == 0 else above)
        net.start(f"b{c}y", lambda f=b_all[c]: f(core), second[c])
        net.start(f"b{c}x", lambda f=b_all[c]: f(core), first[c])
        share(f"b{c}3", b_far[c])
    scale(3)

    def on_columns():
        for c in range(2):
            for k, part in enumerate((b_own, b_down, b_up, b_far)):
                shared(f"b{c}{k}", part[c])

    def on_planes():
        for c in range(2):
            net.arrived(f"a{c}2", a_two[c](core), second[c])
            net.start(f"a{c}u", lambda f=a_all[c]: f(core), above)
            net.start(f"a{c}w", lambda f=a_all[c]: f(core), below)
            share(f"a{c}2", a_two[c])

    def on_planes_shared():
        for c in range(2):
            for k, part in enumerate((a_own, a_one, a_two)):
                shared(f"a{c}{k}", part[c])

    def on_rows():
        for c in range(2):
            net.arrived(f"t{c}2", t_two[c](core), second[c])
            share(f"t{c}2", t_two[c])

    def on_next(c):
        net.arrived(f"a{c}u", a_down[c](core), below)
        if c == 0:
            net.start(f"a{c}f", lambda f=a_down[c]: f(core), above)
        share(f"a{c}3", a_down[c])
        net.arrived(f"a{c}w", a_up[c](core), above)
        if c == 1:
            net.start(f"a{c}f", lambda f=a_up[c]: f(core), below)
        share(f"a{c}4", a_up[c])
        shared(f"a{c}3", a_down[c])
        shared(f"a{c}4", a_up[c])

    def on_one():
        for c in range(2):
            net.arrived(f"b{c}y", b_one[c](core), second[c])
            net.start(f"b{c}z", lambda f=b_one[c]: f(core), first[c])
            share(f"b{c}4", b_one[c])
        for c in range(2):
            shared(f"b{c}4", b_one[c])

    def on_two():
        for c in range(2):
            net.arrived(f"b{c}x", b_two[c](core), first[c])
            share(f"b{c}5", b_two[c])
        for c in range(2):
            shared(f"b{c}5", b_two[c])

    def on_far():
        for c in range(2):
            net.arrived(f"a{c}f", a_far[c](core), below if c == 0 else above)
            share(f"a{c}5", a_far[c])
        for c in range(2):
            shared(f"a{c}5", a_far[c])

    def on_last():
        for c in range(2):
            net.arrived(f"b{c}z", b_last[c](core), first[c])
            share(f"b{c}6", b_last[c])
        for c in range(2):
            shared(f"b{c}6", b_last[c])

    handlers = {
        0: [on_columns],
        1: [on_planes],
        2: [on_planes_shared],
        3: [on_rows],
        4: [lambda: on_next(0)],
        6: [on_one],
        8: [lambda: on_next(1)],
        10: [on_two],
        12: [on_far],
        14: [on_last],
    }
    order = [
        8 + y * 2 + x, 12 + y * 2 + x, z, 4 + z,
        me.down, me.up, 8 + me.oy * 2 + x, 12 + y * 2 + me.ox,
        4 + me.down, 4 + me.up, 8 + y * 2 + me.ox, 12 + me.oy * 2 + x,
        me.far, 4 + me.far, 8 + me.oy * 2 + me.ox, 12 + me.oy * 2 + me.ox,
    ]

    def leave(s, slot):
        return pltpu.make_async_copy(stage.at[slot], kv_ref.at[s], out_sems.at[slot])

    count = math.prod(blocks.shape[1:5])

    def step(s, carry):
        for k, calls in handlers.items():

            @pl.when(s == k)
            def _():
                for call in calls:
                    call()

        which = order[0]
        for k in range(1, steps):
            which = jnp.where(s == k, order[k], which)
        slot = s % 2

        @pl.when(s >= 2)
        def _():
            leave(s - 2, slot).wait()

        block = blocks[which].reshape(count, blocks.shape[5])
        for n in range(4):
            stage[slot, :, n * side : (n + 1) * side] = jnp.dot(
                block, weights[:, n * side : (n + 1) * side], preferred_element_type=jnp.float32
            ).astype(jnp.bfloat16)
        leave(s, slot).start()
        return carry

    lax.fori_loop(0, steps, step, 0)
    for c in range(2):
        for k, part in enumerate((t_own, t_one, t_two)):
            shared(f"t{c}{k}", part[c])
    final = pltpu.make_async_copy(normed, normed_ref, local_sems.at[0])
    final.start()
    leave(steps - 2, 0).wait()
    leave(steps - 1, 1).wait()
    net.drain()
    final.wait()


def gather_and_project(own, rows, key_w, value_w, gain):
    width = own.shape[1]
    piece, share = own.shape[0] // 4, rows.shape[0] // 2
    copies = 58
    return pl.pallas_call(
        gather_kernel,
        out_shape=(
            jax.ShapeDtypeStruct((16, 8 * piece, 4 * HEAD_DIM), jnp.bfloat16),
            jax.ShapeDtypeStruct((2, 2, 2, 2, share, width), jnp.bfloat16),
        ),
        in_specs=[HBM, HBM, HBM, HBM, VMEM],
        out_specs=(HBM, HBM),
        scratch_shapes=[
            pltpu.VMEM((16, 2, 2, 2, piece, width), jnp.bfloat16),
            pltpu.VMEM((2, 2, 2, 2, share, width), jnp.bfloat16),
            pltpu.VMEM((width, 4 * HEAD_DIM), jnp.bfloat16),
            pltpu.VMEM((2, 8 * piece, 4 * HEAD_DIM), jnp.bfloat16),
            pltpu.SemaphoreType.DMA((copies,)),
            pltpu.SemaphoreType.DMA((copies,)),
            pltpu.SemaphoreType.DMA((6,)),
            pltpu.SemaphoreType.DMA((4,)),
            pltpu.SemaphoreType.DMA((2,)),
        ],
        compiler_params=pltpu.CompilerParams(
            collective_id=0, has_side_effects=True, vmem_limit_bytes=48 * MIB
        ),
    )(
        own.reshape(4, piece, width),
        rows.reshape(2, share, width),
        key_w,
        value_w,
        gain,
    )


def attend_kernel(
    layer, group, normed_ref, query_ref, out_ref, kv_ref, temp_ref, partial_ref,
    rows, query_w, out_w, kv, query, total, tops, sums, sems,
):
    y = lax.axis_index("sp") % 2
    count = rows.shape[0]
    wide = group * HEAD_DIM
    chunks = kv.shape[0]
    span = pl.ds(pl.multiple_of(y * wide, wide), wide)
    fetch = [
        pltpu.make_async_copy(normed_ref, rows, sems.at[0]),
        pltpu.make_async_copy(query_ref.at[layer, :, span], query_w, sems.at[1]),
    ]
    held = [
        pltpu.make_async_copy(
            kv_ref.at[j, :, pl.ds(layer * 2 * HEAD_DIM, 2 * HEAD_DIM)], kv.at[j], sems.at[3 + j]
        )
        for j in range(chunks)
    ]
    final = pltpu.make_async_copy(out_ref.at[layer, span, :], out_w, sems.at[2])
    for copy in fetch + held + [final]:
        copy.start()
    for copy in fetch:
        copy.wait()
    for head in range(group):
        scale = temp_ref[layer, y * group + head] * (HEAD_DIM ** (-0.5) * LOG2E)
        query[head] = (
            jnp.dot(
                rows[...],
                query_w[:, head * HEAD_DIM : (head + 1) * HEAD_DIM],
                preferred_element_type=jnp.float32,
            )
            * scale
        ).astype(jnp.bfloat16)
    total[...] = jnp.zeros_like(total)
    sums[...] = jnp.zeros_like(sums)
    tops[...] = jnp.full_like(tops, FLOOR)
    for copy in held:
        copy.wait()

    def step(j, carry):
        for head in range(group):
            scores = lax.dot_general(
                query[head],
                kv[j, :, :HEAD_DIM],
                (((1,), (1,)), ((), ())),
                preferred_element_type=jnp.float32,
            )
            old_top = tops[head, :, :1]
            new_top = jnp.maximum(old_top, jnp.max(scores, axis=-1, keepdims=True))
            shrink = jnp.exp2(old_top - new_top)
            expo = jnp.exp2(scores - new_top)
            tops[head] = jnp.broadcast_to(new_top, tops.shape[1:])
            new_sum = sums[head, :, :1] * shrink + jnp.sum(expo, axis=-1, keepdims=True)
            sums[head] = jnp.broadcast_to(new_sum, sums.shape[1:])
            total[head] = total[head] * shrink + jnp.dot(
                expo.astype(jnp.bfloat16), kv[j, :, HEAD_DIM:], preferred_element_type=jnp.float32
            )
        return carry

    lax.fori_loop(0, chunks, step, 0)
    final.wait()
    attended = jnp.concatenate(
        [(total[head] / sums[head, :, :1]).astype(jnp.bfloat16) for head in range(group)], axis=1
    )
    columns = partial_ref.shape[1]
    for start in range(0, columns, HEAD_DIM):
        block = slice(start, start + HEAD_DIM)
        partial_ref[:, block] = jnp.dot(
            attended, out_w[:, block], preferred_element_type=jnp.float32
        ).astype(jnp.bfloat16)


def attend_layer(layer, group, normed, query_w, out_w, kv, head_temp, chunk=1024):
    count, width = normed.shape
    positions = kv.shape[0] * kv.shape[1]
    chunk = math.gcd(chunk, positions)
    kv = kv.reshape(positions // chunk, chunk, kv.shape[2])
    wide = group * HEAD_DIM
    return pl.pallas_call(
        functools.partial(attend_kernel, layer, group),
        out_shape=jax.ShapeDtypeStruct((count, width), jnp.bfloat16),
        in_specs=[HBM, HBM, HBM, HBM, SMEM],
        out_specs=VMEM,
        scratch_shapes=[
            pltpu.VMEM((count, width), jnp.bfloat16),
            pltpu.VMEM((width, wide), jnp.bfloat16),
            pltpu.VMEM((wide, width), jnp.bfloat16),
            pltpu.VMEM((positions // chunk, chunk, 2 * HEAD_DIM), jnp.bfloat16),
            pltpu.VMEM((group, count, HEAD_DIM), jnp.bfloat16),
            pltpu.VMEM((group, count, HEAD_DIM), jnp.float32),
            pltpu.VMEM((group, count, 128), jnp.float32),
            pltpu.VMEM((group, count, 128), jnp.float32),
            pltpu.SemaphoreType.DMA((3 + positions // chunk,)),
        ],
        compiler_params=pltpu.CompilerParams(vmem_limit_bytes=52 * MIB),
        cost_estimate=pl.CostEstimate(
            flops=4 * count * width * wide + 4 * count * positions * wide,
            bytes_accessed=4 * positions * HEAD_DIM + 4 * width * wide,
            transcendentals=group * count * positions,
        ),
    )(normed, query_w, out_w, kv, head_temp)


def fold_kernel(last, partial_ref, state_ref, gain_ref, *refs):
    if last:
        result_ref, *refs = refs
    else:
        state_out, normed_ref, *refs = refs
    from_core, sums, from_first, relay, from_second, normed, send_sems, recv_sems, local_sem = refs
    me = Place()
    y, x, core = me.y, me.x, me.core
    sibling, xmate, ymate = me.at(core=me.other), me.at(x=me.ox), me.at(y=me.oy)
    first, second = [xmate, ymate], [ymate, xmate]
    greet([sibling, xmate, ymate])
    net = Copies(send_sems, recv_sems)
    sides = [[me.oy, y], [me.ox, x]]

    def piece(ref, c, k, who):
        return ref.at[c, sides[c][k], :, who] if c == 0 else ref.at[c, :, sides[c][k], who]

    for k in range(2):
        for c in range(2):
            net.start(
                f"c{c}{k}",
                lambda c=c, k=k: piece(partial_ref, c, k, me.other),
                sibling,
                lambda c=c, k=k: from_core.at[c, k],
            )
    for k in range(2):
        for c in range(2):
            net.arrived(f"c{c}{k}", from_core.at[c, k], sibling)
            mine = piece(partial_ref, c, k, core)[...]
            sums[c, k] = (
                mine.astype(jnp.float32) + from_core[c, k].astype(jnp.float32)
            ).astype(jnp.bfloat16)
            if k == 0:
                net.start(
                    f"p{c}",
                    lambda c=c: sums.at[c, 0],
                    second[c],
                    lambda c=c: from_first.at[c],
                )
    spots = [(x, me.ox), (y, me.oy)]
    for c in range(2):
        near, far = spots[c]
        net.arrived(f"p{c}", from_first.at[c], second[c])
        relay[c] = (
            sums[c, 1, far].astype(jnp.float32) + from_first[c, far].astype(jnp.float32)
        ).astype(jnp.bfloat16)
        net.start(f"q{c}", lambda c=c: relay.at[c], first[c], lambda c=c: from_second.at[c])
    for c in range(2):
        near, far = spots[c]
        partly = sums[c, 1, near].astype(jnp.float32) + from_first[c, near].astype(jnp.float32)
        net.arrived(f"q{c}", from_second.at[c], first[c])
        state = state_ref[c] + (partly + from_second[c].astype(jnp.float32))
        rows = unit_rows(state) * gain_ref[...]
        if last:
            result_ref[c] = rows
        else:
            state_out[c] = state
            normed[c, y, x, core] = rows.astype(jnp.bfloat16)
            net.start(f"t{c}", lambda c=c: normed.at[c, y, x, core], first[c])
            net.start(f"s{c}0", lambda c=c: normed.at[c, y, x, core], sibling)
    if not last:
        one = [lambda k: normed.at[0, y, me.ox, k], lambda k: normed.at[1, me.oy, x, k]]
        two = [lambda k: normed.at[0, me.oy, :, k], lambda k: normed.at[1, :, me.ox, k]]
        have = [lambda k: normed.at[0, y, :, k], lambda k: normed.at[1, :, x, k]]
        for c in range(2):
            net.arrived(f"t{c}", one[c](core), first[c])
            net.start(f"u{c}", lambda c=c: have[c](core), second[c])
            net.start(f"s{c}1", lambda c=c: one[c](core), sibling)
        for c in range(2):
            net.arrived(f"u{c}", two[c](core), second[c])
            net.start(f"s{c}2", lambda c=c: two[c](core), sibling)
        for c in range(2):
            net.arrived(f"s{c}0", normed.at[c, y, x, me.other], sibling)
            net.arrived(f"s{c}1", one[c](me.other), sibling)
            net.arrived(f"s{c}2", two[c](me.other), sibling)
        copy = pltpu.make_async_copy(normed, normed_ref, local_sem)
        copy.start()
        copy.wait()
    net.drain()


def fold(last, partial, state, gain):
    share, width = state.shape[1:]
    result = jax.ShapeDtypeStruct(state.shape, jnp.float32)
    normed = jax.ShapeDtypeStruct((2, 2, 2, 2, share, width), jnp.bfloat16)
    return pl.pallas_call(
        functools.partial(fold_kernel, last),
        out_shape=result if last else (result, normed),
        in_specs=[VMEM, VMEM, VMEM],
        out_specs=VMEM if last else (VMEM, HBM),
        scratch_shapes=[
            pltpu.VMEM((2, 2, 2, share, width), jnp.bfloat16),
            pltpu.VMEM((2, 2, 2, share, width), jnp.bfloat16),
            pltpu.VMEM((2, 2, share, width), jnp.bfloat16),
            pltpu.VMEM((2, share, width), jnp.bfloat16),
            pltpu.VMEM((2, share, width), jnp.bfloat16),
            pltpu.VMEM((2, 2, 2, 2, share, width), jnp.bfloat16),
            pltpu.SemaphoreType.DMA((20,)),
            pltpu.SemaphoreType.DMA((20,)),
            pltpu.SemaphoreType.DMA,
        ],
        compiler_params=pltpu.CompilerParams(
            collective_id=2 if last else 1, has_side_effects=True, vmem_limit_bytes=32 * MIB
        ),
    )(partial.reshape(2, 2, 2, 2, share, width), state, gain)


def on_planes(
    target, source, target_gain, source_gain, query_w, key_w, value_w, out_w, head_temp, final_gain
):
    width = target.shape[1]
    group = query_w.shape[2] // key_w.shape[2]
    state = target.astype(jnp.float32)
    rows = (unit_rows(state) * target_gain[0].astype(jnp.float32)).astype(jnp.bfloat16)
    kv, normed = gather_and_project(
        unit_rows(source).astype(jnp.bfloat16),
        rows,
        key_w,
        value_w,
        source_gain.astype(jnp.float32)[:, :, None],
    )
    state = state.reshape(2, -1, width)
    for layer in range(2):
        partial = attend_layer(
            layer, group, normed.reshape(-1, width), query_w, out_w, kv, head_temp
        )
        if layer == 0:
            gain = target_gain[1].astype(jnp.float32).reshape(1, width)
            state, normed = fold(False, partial, state, gain)
    gain = final_gain.astype(jnp.float32).reshape(1, width)
    return fold(True, partial, state, gain).reshape(-1, width)


def shifted(block, shift):
    size = lax.axis_size("tp")
    return lax.ppermute(block, "tp", [(i, (i + shift) % size) for i in range(size)])


def gather_rows(block):
    size = lax.axis_size("tp")
    return jnp.concatenate([block] + [shifted(block, k) for k in range(1, size)], axis=0)


def return_rows(blocks):
    size = lax.axis_size("tp")
    count = blocks.shape[0] // size
    mixed = blocks[:count].astype(jnp.float32)
    for k in range(1, size):
        mixed += shifted(blocks[k * count : (k + 1) * count], -k).astype(jnp.float32)
    return mixed


def flash_kernel(rows, query_ref, source_ref, mix_ref, total_ref, top_ref, sum_ref):
    step = pl.program_id(0)
    count = query_ref.shape[0]

    @pl.when(step == 0)
    def _():
        total_ref[...] = jnp.zeros_like(total_ref)
        sum_ref[...] = jnp.zeros_like(sum_ref)
        top_ref[...] = jnp.full_like(top_ref, FLOOR)

    for start in range(0, count, rows):
        block = pl.ds(start, rows)
        scores = lax.dot_general(
            query_ref[block, :],
            source_ref[...],
            (((1,), (1,)), ((), ())),
            preferred_element_type=jnp.float32,
        )
        old_top = top_ref[block, :1]
        new_top = jnp.maximum(old_top, jnp.max(scores, axis=-1, keepdims=True))
        shrink = jnp.exp2(old_top - new_top)
        expo = jnp.exp2(scores - new_top)
        top_ref[block, :] = jnp.broadcast_to(new_top, (rows, top_ref.shape[1]))
        new_sum = sum_ref[block, :1] * shrink + jnp.sum(expo, axis=-1, keepdims=True)
        sum_ref[block, :] = jnp.broadcast_to(new_sum, (rows, sum_ref.shape[1]))
        total_ref[block, :] = total_ref[block, :] * shrink + jnp.dot(
            expo.astype(jnp.bfloat16), source_ref[...], preferred_element_type=jnp.float32
        )

    @pl.when(step == pl.num_programs(0) - 1)
    def _():
        for start in range(0, count, rows):
            block = pl.ds(start, rows)
            mix_ref[block, :] = (total_ref[block, :] / sum_ref[block, :1]).astype(mix_ref.dtype)


def attend(query, source, chunk=CHUNK, rows=ROWS):
    count, width = query.shape
    positions = source.shape[0]
    chunk = math.gcd(chunk, positions)
    rows = math.gcd(rows, count)
    return pl.pallas_call(
        functools.partial(flash_kernel, rows),
        grid=(positions // chunk,),
        out_shape=jax.ShapeDtypeStruct((count, width), jnp.bfloat16),
        in_specs=[
            pl.BlockSpec((count, width), lambda j: (0, 0), pipeline_mode=pl.Buffered(1)),
            pl.BlockSpec((chunk, width), lambda j: (j, 0)),
        ],
        out_specs=pl.BlockSpec((count, width), lambda j: (0, 0), pipeline_mode=pl.Buffered(1)),
        scratch_shapes=[
            pltpu.VMEM((count, width), jnp.float32),
            pltpu.VMEM((count, 128), jnp.float32),
            pltpu.VMEM((count, 128), jnp.float32),
        ],
        compiler_params=pltpu.CompilerParams(
            dimension_semantics=("arbitrary",), vmem_limit_bytes=56 * 1024 * 1024
        ),
        cost_estimate=pl.CostEstimate(
            flops=4 * count * positions * width,
            bytes_accessed=2 * positions * width,
            transcendentals=count * positions,
        ),
    )(query, source)


def per_device(
    target, source, target_gain, source_gain, query_w, key_w, value_w, out_w, head_temp, final_gain
):
    width = target.shape[1]
    heads = query_w.shape[2] // HEAD_DIM
    shared = key_w.shape[2] // HEAD_DIM
    group = heads // shared
    positions = lax.all_gather(
        unit_rows(source).astype(jnp.bfloat16), ("sp", "tp"), axis=0, tiled=True
    )
    hidden_state = target.astype(jnp.float32)
    for layer in range(2):
        gain = source_gain[layer].astype(jnp.float32)
        normed = (unit_rows(hidden_state) * target_gain[layer].astype(jnp.float32)).astype(
            jnp.bfloat16
        )
        queries = jnp.dot(
            gather_rows(normed),
            query_w[layer],
            preferred_element_type=jnp.float32,
        ).astype(jnp.bfloat16)
        count = queries.shape[0]
        scales = head_temp[layer] * (HEAD_DIM ** (-0.5) * LOG2E)
        lifted = []
        for head in range(heads):
            columns = slice((head // group) * HEAD_DIM, (head // group + 1) * HEAD_DIM)
            lifted.append(
                (
                    lax.dot_general(
                        queries[:, head * HEAD_DIM : (head + 1) * HEAD_DIM],
                        key_w[layer][:, columns],
                        (((1,), (1,)), ((), ())),
                        preferred_element_type=jnp.float32,
                    )
                    * (gain * scales[head])
                ).astype(jnp.bfloat16)
            )
        mix = attend(jnp.concatenate(lifted, axis=0), positions)
        attended = []
        for head in range(heads):
            columns = slice((head // group) * HEAD_DIM, (head // group + 1) * HEAD_DIM)
            own = (mix[head * count : (head + 1) * count].astype(jnp.float32) * gain).astype(
                jnp.bfloat16
            )
            attended.append(
                jnp.dot(
                    own, value_w[layer][:, columns], preferred_element_type=jnp.float32
                ).astype(jnp.bfloat16)
            )
        mixed = return_rows(
            jnp.dot(
                jnp.concatenate(attended, axis=1),
                out_w[layer],
                preferred_element_type=jnp.float32,
            ).astype(jnp.bfloat16)
        )
        hidden_state = hidden_state + mixed
    return unit_rows(hidden_state) * final_gain.astype(jnp.float32)


def fits(mesh):
    return dict(mesh.shape) == {"sp": 8, "tp": 4}


def solution(mesh):
    in_specs = (
        P(("sp", "tp"), None),
        P(("sp", "tp"), None),
        P(),
        P(),
        P(None, None, "tp"),
        P(None, None, "tp"),
        P(None, None, "tp"),
        P(None, "tp", None),
        P(None, "tp"),
        P(),
    )
    out_specs = P(("sp", "tp"), None)
    return jax.shard_map(
        on_planes if fits(mesh) else per_device, mesh=mesh, in_specs=in_specs, out_specs=out_specs, check_vma=False
    )
```

```python
import functools
import math

import jax
import jax.numpy as jnp
from jax import lax
from jax.experimental import pallas as pl
from jax.experimental.pallas import tpu as pltpu
from jax.sharding import PartitionSpec as P

HEAD_DIM = 512
EPS = 1e-06
FLOOR = -1e30
CHUNK = 512
ROWS = 512
UNIT = 256
LOG2E = math.log2(math.e)
MESH = pl.DeviceIdType.MESH
MIB = 1024 * 1024
HBM = pl.BlockSpec(memory_space=pl.ANY)
VMEM = pl.BlockSpec(memory_space=pltpu.VMEM)
SMEM = pl.BlockSpec(memory_space=pltpu.SMEM)


def unit_rows(matrix):
    values = matrix.astype(jnp.float32)
    return values * lax.rsqrt(jnp.mean(values * values, axis=-1, keepdims=True) + EPS)


class Place:
    def __init__(self):
        sp, tp = lax.axis_index("sp"), lax.axis_index("tp")
        self.z, self.y = sp // 2, sp % 2
        self.x, self.core = tp // 2, tp % 2
        self.up, self.down = (self.z + 1) % 4, (self.z + 3) % 4
        self.far = (self.z + 2) % 4
        self.ox, self.oy, self.other = 1 - self.x, 1 - self.y, 1 - self.core

    def at(self, z=None, y=None, x=None, core=None):
        z = self.z if z is None else z
        y = self.y if y is None else y
        x = self.x if x is None else x
        core = self.core if core is None else core
        return (z * 2 + y, x * 2 + core)


class Copies:
    def __init__(self, send_sems, recv_sems):
        self.send_sems, self.recv_sems = send_sems, recv_sems
        self.index, self.sent = {}, []

    def _make(self, name, ref, target, dst=None):
        k = self.index.setdefault(name, len(self.index))
        return pltpu.make_async_remote_copy(
            src_ref=ref,
            dst_ref=ref if dst is None else dst,
            send_sem=self.send_sems.at[k],
            recv_sem=self.recv_sems.at[k],
            device_id=target,
            device_id_type=MESH,
        )

    def start(self, name, src, target, dst=None, when=None):
        self.sent.append((name, src, target, dst, when))
        perhaps(when, lambda: self._make(name, src(), target, dst and dst()).start())

    def arrived(self, name, ref, source, when=None):
        perhaps(when, lambda: self._make(name, ref(), source).wait_recv())

    def drain(self):
        for name, src, target, dst, when in self.sent:
            perhaps(when, lambda: self._make(name, src(), target, dst and dst()).wait_send())
        self.sent = []


def perhaps(when, call):
    if when is None:
        call()
    else:
        pl.when(when)(call)


def greet(targets):
    barrier = pltpu.get_barrier_semaphore()
    for target in targets:
        pl.semaphore_signal(barrier, inc=1, device_id=target, device_id_type=MESH)
    pl.semaphore_wait(barrier, len(targets))


def whole_kernel(
    group, source_ref, target_ref, key_ref, value_ref, query_ref, out_ref, source_gain_ref,
    target_gain_ref, final_gain_ref, temp_ref,
    result_ref,
    blocks, normed, weights, small, early, late, query, total, tops, sums, partial, pieces,
    from_core, from_first, from_second, relay, state,
    send_sems, recv_sems, weight_sems,
):
    me = Place()
    z, y, x, core = me.z, me.y, me.x, me.core
    width = weights.shape[0]
    side, wide = HEAD_DIM, group * HEAD_DIM
    steps, positions = blocks.shape[0], math.prod(blocks.shape[1:5])
    share, piece = normed.shape[5], blocks.shape[4]
    count = 16 * share
    span = pl.ds(pl.multiple_of(y * wide, wide), wide)

    def plane(c, zz):
        return blocks.at[c * 4 + zz]

    def column(c, yy, xx):
        return blocks.at[8 + c * 4 + yy * 2 + xx]

    fetches = []
    for layer in range(2):
        for part, ref in enumerate((key_ref, value_ref)):
            n = 2 * layer + part
            fetches.append(
                pltpu.make_async_copy(
                    ref.at[layer, :, pl.ds(pl.multiple_of(y * side, side), side)],
                    weights.at[:, pl.ds(n * side, side)],
                    weight_sems.at[n],
                )
            )

    def query_fetch(layer, dst, sem):
        return [pltpu.make_async_copy(query_ref.at[layer, :, span], dst, weight_sems.at[sem])]

    def out_fetch(layer, dst, sem):
        half = width // 2
        return [
            pltpu.make_async_copy(
                out_ref.at[layer, span, pl.ds(k * half, half)],
                dst.at[pl.ds(k * half, half)],
                weight_sems.at[sem + k],
            )
            for k in range(2)
        ]

    late_query, late_out = weights.at[:, pl.ds(0, wide)], weights.at[:, pl.ds(wide, wide)]
    query_0, out_0 = query_fetch(0, small, 4), out_fetch(0, small, 5)
    query_1, out_1 = query_fetch(1, late_query, 7), out_fetch(1, late_out, 8)

    def begin(copies):
        for copy in copies:
            copy.start()

    def finish(copies):
        for copy in copies:
            copy.wait()

    begin(fetches)
    begin(query_0)
    for c in range(2):
        blocks[c * 4 + z, y, x, core] = unit_rows(source_ref[c]).astype(jnp.bfloat16)
        blocks[8 + c * 4 + y * 2 + x, z // 2, z % 2, core] = unit_rows(source_ref[2 + c]).astype(
            jnp.bfloat16
        )
        rows = target_ref[c].astype(jnp.float32)
        state[c] = rows
        normed[0, c, y, x, core] = (unit_rows(rows) * target_gain_ref[0:1]).astype(jnp.bfloat16)
    greet([me.at(x=me.ox), me.at(y=me.oy), me.at(z=me.up), me.at(z=me.down), me.at(core=me.other)])

    net = Copies(send_sems, recv_sems)
    sibling, xmate, ymate = me.at(core=me.other), me.at(x=me.ox), me.at(y=me.oy)
    above, below = me.at(z=me.up), me.at(z=me.down)
    first, second = [xmate, ymate], [ymate, xmate]

    def share_with(name, part, when=None):
        net.start(name + "d", lambda: part(core), sibling, when=when)

    def shared(name, part, when=None):
        net.arrived(name + "d", lambda: part(me.other), sibling, when=when)

    def pair(c, zz):
        return lambda k: plane(c, zz).at[y, :, k] if c == 0 else plane(c, zz).at[:, x, k]

    def mates(c, zz):
        return lambda k: plane(c, zz).at[me.oy, :, k] if c == 0 else plane(c, zz).at[:, me.ox, k]

    def spot(c, zz):
        return lambda k: column(c, y, x).at[zz // 2, zz % 2, k]

    def whole(c, yy, xx):
        return lambda k: column(c, yy, xx).at[:, :, k]

    a_own = [lambda k, c=c: plane(c, z).at[y, x, k] for c in range(2)]
    a_one = [lambda k: plane(0, z).at[y, me.ox, k], lambda k: plane(1, z).at[me.oy, x, k]]
    b_one = [whole(0, me.oy, x), whole(1, y, me.ox)]
    b_two = [whole(0, y, me.ox), whole(1, me.oy, x)]
    b_last = [whole(c, me.oy, me.ox) for c in range(2)]
    t_own = [lambda k, c=c: normed.at[0, c, y, x, k] for c in range(2)]
    t_one = [lambda k: normed.at[0, 0, y, me.ox, k], lambda k: normed.at[0, 1, me.oy, x, k]]
    t_two = [lambda k: normed.at[0, 0, me.oy, :, k], lambda k: normed.at[0, 1, :, me.ox, k]]
    t_have = [lambda k: normed.at[0, 0, y, :, k], lambda k: normed.at[0, 1, :, x, k]]
    top = 3
    hops = range(top + 1)
    ways = {
        "u": (below, above, [z - d for d in hops], [z >= d for d in hops]),
        "w": (above, below, [z + d for d in hops], [z + d <= top for d in hops]),
    }
    more = {"u": z < top, "w": z > 0}
    goes = {way: [jnp.logical_and(c, more[way]) for c in ways[way][3]] for way in ways}

    def go(c, part, name):
        for way, (_, ahead, _, _) in ways.items():
            net.start(f"{name}{c}{way}1", lambda: part(core), ahead, when=more[way])

    def pass_on(c, d, name, region):
        for way, (behind, ahead, began, comes) in ways.items():
            part = region(c, began[d])
            net.arrived(f"{name}{c}{way}{d}", lambda: part(core), behind, when=comes[d])
            if d < top:
                net.start(
                    f"{name}{c}{way}{d + 1}",
                    lambda part=part: part(core),
                    ahead,
                    when=goes[way][d],
                )
            if name == "a":
                net.start(
                    f"a{c}{way}{d}m", lambda part=part: part(core), second[c], when=comes[d]
                )
            share_with(f"{name}{c}{way}{d}", part, when=comes[d])

    for c in range(2):
        net.start(f"a{c}1", lambda c=c: a_own[c](core), first[c])
        go(c, spot(c, z), "b")
    for c in range(2):
        net.start(f"t{c}1", lambda c=c: t_own[c](core), first[c])
        share_with(f"b{c}0", spot(c, z))
        share_with(f"t{c}0", t_own[c])

    def scale(n):
        fetches[n].wait()
        columns = pl.ds(n * side, side)

        def body(i, carry):
            block = pl.ds(i * 256, 256)
            weights[block, columns] = (
                weights[block, columns].astype(jnp.float32) * source_gain_ref[n // 2, block, :]
            ).astype(jnp.bfloat16)
            return carry

        lax.fori_loop(0, width // 256, body, 0)

    def own_planes():
        for c in range(2):
            net.arrived(f"a{c}m", lambda: mates(c, z)(core), second[c])
            share_with(f"a{c}m", mates(c, z))
        for c in range(2):
            shared(f"a{c}0", pair(c, z))
            shared(f"a{c}m", mates(c, z))

    def planes_come(d):
        for c in range(2):
            pass_on(c, d, "a", pair)

    def planes_done(d):
        for c in range(2):
            for way, (_, _, began, comes) in ways.items():
                part = mates(c, began[d])
                net.arrived(f"a{c}{way}{d}m", lambda: part(core), second[c], when=comes[d])
                share_with(f"a{c}{way}{d}m", part, when=comes[d])
        for c in range(2):
            for way, (_, _, began, comes) in ways.items():
                shared(f"a{c}{way}{d}", pair(c, began[d]), when=comes[d])
                shared(f"a{c}{way}{d}m", mates(c, began[d]), when=comes[d])

    def rows_done():
        for c in range(2):
            net.arrived(f"t{c}2", lambda: t_two[c](core), second[c])
            share_with(f"t{c}2", t_two[c])

    def columns_come(d):
        for c in range(2):
            pass_on(c, d, "b", spot)

    def columns_go(name, targets):
        for c in range(2):
            part = whole(c, y, x)
            net.start(f"b{c}{name}", lambda part=part: part(core), targets[c])

    def columns_done():
        for c in range(2):
            shared(f"b{c}0", spot(c, z))
            for d in range(1, top + 1):
                for way, (_, _, began, comes) in ways.items():
                    shared(f"b{c}{way}{d}", spot(c, began[d]), when=comes[d])

    def columns_one():
        for c in range(2):
            net.arrived(f"b{c}y", lambda: b_one[c](core), second[c])
            share_with(f"b{c}4", b_one[c])
        for c in range(2):
            shared(f"b{c}4", b_one[c])

    def columns_relay():
        for c in range(2):
            net.start(f"b{c}z", lambda c=c: b_one[c](core), first[c])

    def columns_two():
        for c in range(2):
            net.arrived(f"b{c}x", lambda: b_two[c](core), first[c])
            share_with(f"b{c}5", b_two[c])
        for c in range(2):
            shared(f"b{c}5", b_two[c])

    def columns_last():
        for c in range(2):
            net.arrived(f"b{c}z", lambda: b_last[c](core), first[c])
            share_with(f"b{c}6", b_last[c])
        for c in range(2):
            shared(f"b{c}6", b_last[c])

    scale(0)
    scale(1)
    scale(2)
    for c in range(2):
        net.arrived(f"a{c}1", lambda: a_one[c](core), first[c])
        part = pair(c, z)
        net.start(f"a{c}m", lambda part=part: part(core), second[c])
        share_with(f"a{c}0", part)
    columns_come(1)
    for c in range(2):
        net.arrived(f"t{c}1", lambda: t_one[c](core), first[c])
        net.start(f"t{c}2", lambda c=c: t_have[c](core), second[c])
        share_with(f"t{c}1", t_one[c])
    columns_come(2)
    for c in range(2):
        go(c, pair(c, z), "a")
    scale(3)

    def project_rows(layer, ref):
        rows = normed[layer].reshape(count, width)
        for head in range(group):
            factor = temp_ref[layer, y * group + head] * (HEAD_DIM ** (-0.5) * LOG2E)
            query[head] = (
                jnp.dot(
                    rows,
                    ref[:, head * side : (head + 1) * side],
                    preferred_element_type=jnp.float32,
                )
                * factor
            ).astype(jnp.bfloat16)
        total[...] = jnp.zeros_like(total)
        sums[...] = jnp.zeros_like(sums)
        tops[...] = jnp.full_like(tops, FLOOR)

    def attend(kv):
        keys = kv[:, :, :side].reshape(-1, side)
        values = kv[:, :, side:].reshape(-1, side)
        units = [(head, pl.ds(r, UNIT)) for head in range(group) for r in range(0, count, UNIT)]

        def score(head, block):
            return lax.dot_general(
                query[head, block],
                keys,
                (((1,), (1,)), ((), ())),
                preferred_element_type=jnp.float32,
            )

        ahead = score(*units[0])
        for k, (head, block) in enumerate(units):
            scores = ahead
            if k + 1 < len(units):
                ahead = score(*units[k + 1])
            old_top = tops[head, block, :1]
            new_top = jnp.maximum(old_top, jnp.max(scores, axis=-1, keepdims=True))
            shrink = jnp.exp2(old_top - new_top)
            expo = jnp.exp2(scores - new_top)
            tops[head, block] = jnp.broadcast_to(new_top, (UNIT, tops.shape[2]))
            new_sum = sums[head, block, :1] * shrink + jnp.sum(expo, axis=-1, keepdims=True)
            sums[head, block] = jnp.broadcast_to(new_sum, (UNIT, sums.shape[2]))
            total[head, block] = total[head, block] * shrink + jnp.dot(
                expo.astype(jnp.bfloat16), values, preferred_element_type=jnp.float32
            )

    def first_query():
        rows_done()
        for c in range(2):
            for k, part in enumerate((t_own, t_one, t_two)):
                shared(f"t{c}{k}", part[c])
        finish(query_0)
        project_rows(0, small)
        begin(out_0)

    handlers = {
        0: [own_planes],
        1: [lambda: columns_come(3), lambda: columns_go("y", second), first_query],
        2: [columns_done],
        3: [lambda: planes_come(1)],
        4: [lambda: columns_go("x", first), columns_one],
        6: [lambda: planes_come(2), lambda: planes_done(1)],
        8: [columns_two],
        9: [lambda: planes_come(3), columns_relay],
        10: [lambda: planes_done(2)],
        12: [lambda: planes_done(3)],
        14: [columns_last],
    }
    low = z < 2
    near = jnp.where(z == 0, 1, jnp.where(z == 1, 0, jnp.where(z == 2, 3, 2)))
    next_one = jnp.where(low, 2, 1)
    far = jnp.where(low, 3, 0)
    order = [
        z, 4 + z, 8 + y * 2 + x, 12 + y * 2 + x,
        8 + me.oy * 2 + x, 12 + y * 2 + me.ox, near, 4 + near,
        8 + y * 2 + me.ox, 12 + me.oy * 2 + x, next_one, 4 + next_one,
        far, 4 + far, 8 + me.oy * 2 + me.ox, 12 + me.oy * 2 + me.ox,
    ]

    def step(s, carry):
        for k, calls in handlers.items():

            @pl.when(s == k)
            def _():
                for call in calls:
                    call()

        which = order[0]
        for k in range(1, steps):
            which = jnp.where(s == k, order[k], which)
        block = blocks[which].reshape(positions, width)
        for n in range(4):
            made = jnp.dot(
                block, weights[:, n * side : (n + 1) * side], preferred_element_type=jnp.float32
            ).astype(jnp.bfloat16)
            if n < 2:
                early[s % 2, :, n * side : (n + 1) * side] = made
            else:
                late[s, :, (n - 2) * side : (n - 1) * side] = made

        @pl.when(s % 2 == 1)
        def _():
            attend(early)

        return carry

    lax.fori_loop(0, steps, step, 0)
    begin(query_1)
    begin(out_1)

    def out_rows(layer, ref, c):
        block = slice(c * (count // 2), (c + 1) * (count // 2))
        attended = jnp.concatenate(
            [
                (total[head, block] / sums[head, block, :1]).astype(jnp.bfloat16)
                for head in range(group)
            ],
            axis=1,
        )
        half = width // 2
        for k in range(2):
            for n in range(0, half, side):
                term = jnp.dot(
                    attended,
                    ref[k * half : (k + 1) * half, n : n + side],
                    preferred_element_type=jnp.float32,
                ).astype(jnp.bfloat16)
                partial[c, :, :, :, :, k * half + n : k * half + n + side] = term.reshape(
                    2, 2, 2, share, side
                )

    sides = [[me.oy, y], [me.ox, x]]
    spots = [(x, me.ox), (y, me.oy)]

    def piece_of(c, k, who):
        return partial.at[c, sides[c][k], :, who] if c == 0 else partial.at[c, :, sides[c][k], who]

    def fold_start(layer, c):
        for k in range(2):
            net.start(
                f"c{c}{k}{layer}",
                lambda c=c, k=k: piece_of(c, k, me.other),
                sibling,
                lambda c=c, k=k: from_core.at[layer, c, k],
            )

    def fold_pairs(layer):
        for k in range(2):
            for c in range(2):
                net.arrived(f"c{c}{k}{layer}", lambda: from_core.at[layer, c, k], sibling)
                pieces[c, k] = (
                    piece_of(c, k, core)[...].astype(jnp.float32)
                    + from_core[layer, c, k].astype(jnp.float32)
                ).astype(jnp.bfloat16)
                if k == 0:
                    net.start(
                        f"p{c}{layer}",
                        lambda c=c: pieces.at[c, 0],
                        second[c],
                        lambda c=c: from_first.at[layer, c],
                    )
        for c in range(2):
            far = spots[c][1]
            net.arrived(f"p{c}{layer}", lambda: from_first.at[layer, c], second[c])
            relay[c] = (
                pieces[c, 1, far].astype(jnp.float32) + from_first[layer, c, far].astype(jnp.float32)
            ).astype(jnp.bfloat16)
            net.start(
                f"q{c}{layer}",
                lambda c=c: relay.at[c],
                first[c],
                lambda c=c: from_second.at[layer, c],
            )

    def folded(layer, c):
        near = spots[c][0]
        partly = pieces[c, 1, near].astype(jnp.float32) + from_first[layer, c, near].astype(
            jnp.float32
        )
        net.arrived(f"q{c}{layer}", lambda: from_second.at[layer, c], first[c])
        return state[c] + (partly + from_second[layer, c].astype(jnp.float32))

    finish(out_0)
    for c in range(2):
        out_rows(0, small, c)
        fold_start(0, c)
    fold_pairs(0)
    own = [lambda k, c=c: normed.at[1, c, y, x, k] for c in range(2)]
    one = [lambda k: normed.at[1, 0, y, me.ox, k], lambda k: normed.at[1, 1, me.oy, x, k]]
    two = [lambda k: normed.at[1, 0, me.oy, :, k], lambda k: normed.at[1, 1, :, me.ox, k]]
    have = [lambda k: normed.at[1, 0, y, :, k], lambda k: normed.at[1, 1, :, x, k]]
    for c in range(2):
        rows = folded(0, c)
        state[c] = rows
        normed[1, c, y, x, core] = (unit_rows(rows) * target_gain_ref[1:2]).astype(jnp.bfloat16)
        net.start(f"n{c}1", lambda c=c: own[c](core), first[c])
        share_with(f"n{c}0", own[c])
    for c in range(2):
        net.arrived(f"n{c}1", lambda: one[c](core), first[c])
        net.start(f"n{c}2", lambda c=c: have[c](core), second[c])
        share_with(f"n{c}1", one[c])
    for c in range(2):
        net.arrived(f"n{c}2", lambda: two[c](core), second[c])
        share_with(f"n{c}2", two[c])
    for c in range(2):
        for k, part in enumerate((own, one, two)):
            shared(f"n{c}{k}", part[c])
    net.drain()
    finish(query_1)
    project_rows(1, late_query)

    def second_step(j, carry):
        attend(late.at[pl.ds(4 * j, 4)])
        return carry

    lax.fori_loop(0, steps // 4, second_step, 0)
    finish(out_1)
    for c in range(2):
        out_rows(1, late_out, c)
        fold_start(1, c)
    fold_pairs(1)
    for c in range(2):
        result_ref[c] = unit_rows(folded(1, c)) * final_gain_ref[...]
    net.drain()


def on_planes(
    target, source, target_gain, source_gain, query_w, key_w, value_w, out_w, head_temp, final_gain
):
    width = target.shape[1]
    group = query_w.shape[2] // key_w.shape[2]
    piece, share = source.shape[0] // 4, target.shape[0] // 2
    count, positions, copies = 16 * share, 8 * piece, 140
    part = (2, share, width)
    return pl.pallas_call(
        functools.partial(whole_kernel, group),
        out_shape=jax.ShapeDtypeStruct(part, jnp.float32),
        in_specs=[VMEM, VMEM, HBM, HBM, HBM, HBM, VMEM, VMEM, VMEM, SMEM],
        out_specs=VMEM,
        scratch_shapes=[
            pltpu.VMEM((16, 2, 2, 2, piece, width), jnp.bfloat16),
            pltpu.VMEM((2, 2, 2, 2, 2, share, width), jnp.bfloat16),
            pltpu.VMEM((width, 4 * HEAD_DIM), jnp.bfloat16),
            pltpu.VMEM((width, group * HEAD_DIM), jnp.bfloat16),
            pltpu.VMEM((2, positions, 2 * HEAD_DIM), jnp.bfloat16),
            pltpu.VMEM((16, positions, 2 * HEAD_DIM), jnp.bfloat16),
            pltpu.VMEM((group, count, HEAD_DIM), jnp.bfloat16),
            pltpu.VMEM((group, count, HEAD_DIM), jnp.float32),
            pltpu.VMEM((group, count, 128), jnp.float32),
            pltpu.VMEM((group, count, 128), jnp.float32),
            pltpu.VMEM((2, 2, 2, 2, share, width), jnp.bfloat16),
            pltpu.VMEM((2, 2, 2, share, width), jnp.bfloat16),
            pltpu.VMEM((2, 2, 2, 2, share, width), jnp.bfloat16),
            pltpu.VMEM((2, 2, 2, share, width), jnp.bfloat16),
            pltpu.VMEM((2, 2, share, width), jnp.bfloat16),
            pltpu.VMEM((2, share, width), jnp.bfloat16),
            pltpu.VMEM(part, jnp.float32),
            pltpu.SemaphoreType.DMA((copies,)),
            pltpu.SemaphoreType.DMA((copies,)),
            pltpu.SemaphoreType.DMA((10,)),
        ],
        compiler_params=pltpu.CompilerParams(
            collective_id=0, has_side_effects=True, vmem_limit_bytes=63 * MIB
        ),
    )(
        source.reshape(4, piece, width),
        target.reshape(2, share, width),
        key_w,
        value_w,
        query_w,
        out_w,
        source_gain.astype(jnp.float32)[:, :, None],
        target_gain.astype(jnp.float32),
        final_gain.astype(jnp.float32).reshape(1, width),
        head_temp,
    ).reshape(-1, width)


def shifted(block, shift):
    size = lax.axis_size("tp")
    return lax.ppermute(block, "tp", [(i, (i + shift) % size) for i in range(size)])


def gather_rows(block):
    size = lax.axis_size("tp")
    return jnp.concatenate([block] + [shifted(block, k) for k in range(1, size)], axis=0)


def return_rows(blocks):
    size = lax.axis_size("tp")
    count = blocks.shape[0] // size
    mixed = blocks[:count].astype(jnp.float32)
    for k in range(1, size):
        mixed += shifted(blocks[k * count : (k + 1) * count], -k).astype(jnp.float32)
    return mixed


def flash_kernel(rows, query_ref, source_ref, mix_ref, total_ref, top_ref, sum_ref):
    step = pl.program_id(0)
    count = query_ref.shape[0]

    @pl.when(step == 0)
    def _():
        total_ref[...] = jnp.zeros_like(total_ref)
        sum_ref[...] = jnp.zeros_like(sum_ref)
        top_ref[...] = jnp.full_like(top_ref, FLOOR)

    for start in range(0, count, rows):
        block = pl.ds(start, rows)
        scores = lax.dot_general(
            query_ref[block, :],
            source_ref[...],
            (((1,), (1,)), ((), ())),
            preferred_element_type=jnp.float32,
        )
        old_top = top_ref[block, :1]
        new_top = jnp.maximum(old_top, jnp.max(scores, axis=-1, keepdims=True))
        shrink = jnp.exp2(old_top - new_top)
        expo = jnp.exp2(scores - new_top)
        top_ref[block, :] = jnp.broadcast_to(new_top, (rows, top_ref.shape[1]))
        new_sum = sum_ref[block, :1] * shrink + jnp.sum(expo, axis=-1, keepdims=True)
        sum_ref[block, :] = jnp.broadcast_to(new_sum, (rows, sum_ref.shape[1]))
        total_ref[block, :] = total_ref[block, :] * shrink + jnp.dot(
            expo.astype(jnp.bfloat16), source_ref[...], preferred_element_type=jnp.float32
        )

    @pl.when(step == pl.num_programs(0) - 1)
    def _():
        for start in range(0, count, rows):
            block = pl.ds(start, rows)
            mix_ref[block, :] = (total_ref[block, :] / sum_ref[block, :1]).astype(mix_ref.dtype)


def attend(query, source, chunk=CHUNK, rows=ROWS):
    count, width = query.shape
    positions = source.shape[0]
    chunk = math.gcd(chunk, positions)
    rows = math.gcd(rows, count)
    return pl.pallas_call(
        functools.partial(flash_kernel, rows),
        grid=(positions // chunk,),
        out_shape=jax.ShapeDtypeStruct((count, width), jnp.bfloat16),
        in_specs=[
            pl.BlockSpec((count, width), lambda j: (0, 0), pipeline_mode=pl.Buffered(1)),
            pl.BlockSpec((chunk, width), lambda j: (j, 0)),
        ],
        out_specs=pl.BlockSpec((count, width), lambda j: (0, 0), pipeline_mode=pl.Buffered(1)),
        scratch_shapes=[
            pltpu.VMEM((count, width), jnp.float32),
            pltpu.VMEM((count, 128), jnp.float32),
            pltpu.VMEM((count, 128), jnp.float32),
        ],
        compiler_params=pltpu.CompilerParams(
            dimension_semantics=("arbitrary",), vmem_limit_bytes=56 * 1024 * 1024
        ),
        cost_estimate=pl.CostEstimate(
            flops=4 * count * positions * width,
            bytes_accessed=2 * positions * width,
            transcendentals=count * positions,
        ),
    )(query, source)


def per_device(
    target, source, target_gain, source_gain, query_w, key_w, value_w, out_w, head_temp, final_gain
):
    width = target.shape[1]
    heads = query_w.shape[2] // HEAD_DIM
    shared = key_w.shape[2] // HEAD_DIM
    group = heads // shared
    positions = lax.all_gather(
        unit_rows(source).astype(jnp.bfloat16), ("sp", "tp"), axis=0, tiled=True
    )
    hidden_state = target.astype(jnp.float32)
    for layer in range(2):
        gain = source_gain[layer].astype(jnp.float32)
        normed = (unit_rows(hidden_state) * target_gain[layer].astype(jnp.float32)).astype(
            jnp.bfloat16
        )
        queries = jnp.dot(
            gather_rows(normed),
            query_w[layer],
            preferred_element_type=jnp.float32,
        ).astype(jnp.bfloat16)
        count = queries.shape[0]
        scales = head_temp[layer] * (HEAD_DIM ** (-0.5) * LOG2E)
        lifted = []
        for head in range(heads):
            columns = slice((head // group) * HEAD_DIM, (head // group + 1) * HEAD_DIM)
            lifted.append(
                (
                    lax.dot_general(
                        queries[:, head * HEAD_DIM : (head + 1) * HEAD_DIM],
                        key_w[layer][:, columns],
                        (((1,), (1,)), ((), ())),
                        preferred_element_type=jnp.float32,
                    )
                    * (gain * scales[head])
                ).astype(jnp.bfloat16)
            )
        mix = attend(jnp.concatenate(lifted, axis=0), positions)
        attended = []
        for head in range(heads):
            columns = slice((head // group) * HEAD_DIM, (head // group + 1) * HEAD_DIM)
            own = (mix[head * count : (head + 1) * count].astype(jnp.float32) * gain).astype(
                jnp.bfloat16
            )
            attended.append(
                jnp.dot(
                    own, value_w[layer][:, columns], preferred_element_type=jnp.float32
                ).astype(jnp.bfloat16)
            )
        mixed = return_rows(
            jnp.dot(
                jnp.concatenate(attended, axis=1),
                out_w[layer],
                preferred_element_type=jnp.float32,
            ).astype(jnp.bfloat16)
        )
        hidden_state = hidden_state + mixed
    return unit_rows(hidden_state) * final_gain.astype(jnp.float32)


def fits(mesh):
    return dict(mesh.shape) == {"sp": 8, "tp": 4}


def solution(mesh):
    in_specs = (
        P(("sp", "tp"), None),
        P(("sp", "tp"), None),
        P(),
        P(),
        P(None, None, "tp"),
        P(None, None, "tp"),
        P(None, None, "tp"),
        P(None, "tp", None),
        P(None, "tp"),
        P(),
    )
    out_specs = P(("sp", "tp"), None)
    return jax.shard_map(
        on_planes if fits(mesh) else per_device, mesh=mesh, in_specs=in_specs, out_specs=out_specs, check_vma=False
    )
```

```python
import functools
import math

import jax
import jax.numpy as jnp
from jax import lax
from jax.experimental import pallas as pl
from jax.experimental.pallas import tpu as pltpu
from jax.sharding import PartitionSpec as P

HEAD_DIM = 512
EPS = 1e-06
FLOOR = -1e30
CHUNK = 512
ROWS = 512
UNIT = 256
LOG2E = math.log2(math.e)
LATER = 12
MESH = pl.DeviceIdType.MESH
MIB = 1024 * 1024
HBM = pl.BlockSpec(memory_space=pl.ANY)
VMEM = pl.BlockSpec(memory_space=pltpu.VMEM)
SMEM = pl.BlockSpec(memory_space=pltpu.SMEM)


def unit_rows(matrix):
    values = matrix.astype(jnp.float32)
    return values * lax.rsqrt(jnp.mean(values * values, axis=-1, keepdims=True) + EPS)


class Place:
    def __init__(self):
        sp, tp = lax.axis_index("sp"), lax.axis_index("tp")
        self.z, self.y = sp // 2, sp % 2
        self.x, self.core = tp // 2, tp % 2
        self.up, self.down = (self.z + 1) % 4, (self.z + 3) % 4
        self.far = (self.z + 2) % 4
        self.ox, self.oy, self.other = 1 - self.x, 1 - self.y, 1 - self.core

    def at(self, z=None, y=None, x=None, core=None):
        z = self.z if z is None else z
        y = self.y if y is None else y
        x = self.x if x is None else x
        core = self.core if core is None else core
        return (z * 2 + y, x * 2 + core)


class Copies:
    def __init__(self, send_sems, recv_sems):
        self.send_sems, self.recv_sems = send_sems, recv_sems
        self.index, self.sent = {}, []

    def _make(self, name, ref, target, dst=None):
        k = self.index.setdefault(name, len(self.index))
        return pltpu.make_async_remote_copy(
            src_ref=ref,
            dst_ref=ref if dst is None else dst,
            send_sem=self.send_sems.at[k],
            recv_sem=self.recv_sems.at[k],
            device_id=target,
            device_id_type=MESH,
        )

    def start(self, name, src, target, dst=None, when=None):
        self.sent.append((name, src, target, dst, when))
        perhaps(when, lambda: self._make(name, src(), target, dst and dst()).start())

    def arrived(self, name, ref, source, when=None):
        perhaps(when, lambda: self._make(name, ref(), source).wait_recv())

    def drain(self):
        for name, src, target, dst, when in self.sent:
            perhaps(when, lambda: self._make(name, src(), target, dst and dst()).wait_send())
        self.sent = []


def perhaps(when, call):
    if when is None:
        call()
    else:
        pl.when(when)(call)


def greet(targets):
    barrier = pltpu.get_barrier_semaphore()
    for target in targets:
        pl.semaphore_signal(barrier, inc=1, device_id=target, device_id_type=MESH)
    pl.semaphore_wait(barrier, len(targets))


def whole_kernel(
    group, source_ref, target_ref, key_ref, value_ref, query_ref, out_ref, source_gain_ref,
    target_gain_ref, final_gain_ref, temp_ref,
    result_ref,
    blocks, normed, weights, small, early, late, query, total, tops, sums, partial, pieces,
    from_core, from_first, from_second, relay, state,
    send_sems, recv_sems, weight_sems,
):
    me = Place()
    z, y, x, core = me.z, me.y, me.x, me.core
    width = weights.shape[0]
    side, wide = HEAD_DIM, group * HEAD_DIM
    steps, positions = blocks.shape[0], math.prod(blocks.shape[1:5])
    share, piece = normed.shape[5], blocks.shape[4]
    count = 16 * share
    span = pl.ds(pl.multiple_of(y * wide, wide), wide)

    def plane(c, zz):
        return blocks.at[c * 4 + zz]

    def column(c, yy, xx):
        return blocks.at[8 + c * 4 + yy * 2 + xx]

    fetches = []
    for layer in range(2):
        for part, ref in enumerate((key_ref, value_ref)):
            n = 2 * layer + part
            fetches.append(
                pltpu.make_async_copy(
                    ref.at[layer, :, pl.ds(pl.multiple_of(y * side, side), side)],
                    weights.at[:, pl.ds(n * side, side)],
                    weight_sems.at[n],
                )
            )

    def query_fetch(layer, dst, sem):
        return [pltpu.make_async_copy(query_ref.at[layer, :, span], dst, weight_sems.at[sem])]

    def out_fetch(layer, dst, sem):
        half = width // 2
        return [
            pltpu.make_async_copy(
                out_ref.at[layer, span, pl.ds(k * half, half)],
                dst.at[pl.ds(k * half, half)],
                weight_sems.at[sem + k],
            )
            for k in range(2)
        ]

    late_query, late_out = weights.at[:, pl.ds(0, wide)], weights.at[:, pl.ds(wide, wide)]
    query_0, out_0 = query_fetch(0, small, 4), out_fetch(0, small, 5)
    query_1, out_1 = query_fetch(1, late_query, 7), out_fetch(1, late_out, 8)

    def begin(copies):
        for copy in copies:
            copy.start()

    def finish(copies):
        for copy in copies:
            copy.wait()

    target_gain = target_gain_ref[...].astype(jnp.float32)
    begin(fetches)
    begin(query_0)
    for c in range(2):
        of_plane = source_ref[c * piece : (c + 1) * piece]
        of_column = source_ref[(2 + c) * piece : (3 + c) * piece]
        blocks[c * 4 + z, y, x, core] = unit_rows(of_plane).astype(jnp.bfloat16)
        blocks[8 + c * 4 + y * 2 + x, z // 2, z % 2, core] = unit_rows(of_column).astype(
            jnp.bfloat16
        )
        rows = target_ref[c * share : (c + 1) * share].astype(jnp.float32)
        state[c] = rows
        normed[0, c, y, x, core] = (unit_rows(rows) * target_gain[0:1]).astype(jnp.bfloat16)
    greet([me.at(x=me.ox), me.at(y=me.oy), me.at(z=me.up), me.at(z=me.down), me.at(core=me.other)])

    net = Copies(send_sems, recv_sems)
    sibling, xmate, ymate = me.at(core=me.other), me.at(x=me.ox), me.at(y=me.oy)
    above, below = me.at(z=me.up), me.at(z=me.down)
    first, second = [xmate, ymate], [ymate, xmate]

    def share_with(name, part, when=None):
        net.start(name + "d", lambda: part(core), sibling, when=when)

    def shared(name, part, when=None):
        net.arrived(name + "d", lambda: part(me.other), sibling, when=when)

    def pair(c, zz):
        return lambda k: plane(c, zz).at[y, :, k] if c == 0 else plane(c, zz).at[:, x, k]

    def mates(c, zz):
        return lambda k: plane(c, zz).at[me.oy, :, k] if c == 0 else plane(c, zz).at[:, me.ox, k]

    def spot(c, zz):
        return lambda k: column(c, y, x).at[zz // 2, zz % 2, k]

    def whole(c, yy, xx):
        return lambda k: column(c, yy, xx).at[:, :, k]

    a_own = [lambda k, c=c: plane(c, z).at[y, x, k] for c in range(2)]
    a_one = [lambda k: plane(0, z).at[y, me.ox, k], lambda k: plane(1, z).at[me.oy, x, k]]
    b_one = [whole(0, me.oy, x), whole(1, y, me.ox)]
    b_two = [whole(0, y, me.ox), whole(1, me.oy, x)]
    b_last = [whole(c, me.oy, me.ox) for c in range(2)]
    t_own = [lambda k, c=c: normed.at[0, c, y, x, k] for c in range(2)]
    t_one = [lambda k: normed.at[0, 0, y, me.ox, k], lambda k: normed.at[0, 1, me.oy, x, k]]
    t_two = [lambda k: normed.at[0, 0, me.oy, :, k], lambda k: normed.at[0, 1, :, me.ox, k]]
    t_have = [lambda k: normed.at[0, 0, y, :, k], lambda k: normed.at[0, 1, :, x, k]]
    top = 3
    hops = range(top + 1)
    ways = {
        "u": (below, above, [z - d for d in hops], [z >= d for d in hops]),
        "w": (above, below, [z + d for d in hops], [z + d <= top for d in hops]),
    }
    more = {"u": z < top, "w": z > 0}
    goes = {way: [jnp.logical_and(c, more[way]) for c in ways[way][3]] for way in ways}

    def go(c, part, name):
        for way, (_, ahead, _, _) in ways.items():
            net.start(f"{name}{c}{way}1", lambda: part(core), ahead, when=more[way])

    def pass_on(c, d, name, region):
        for way, (behind, ahead, began, comes) in ways.items():
            part = region(c, began[d])
            net.arrived(f"{name}{c}{way}{d}", lambda: part(core), behind, when=comes[d])
            if d < top:
                net.start(
                    f"{name}{c}{way}{d + 1}",
                    lambda part=part: part(core),
                    ahead,
                    when=goes[way][d],
                )
            if name == "a":
                net.start(
                    f"a{c}{way}{d}m", lambda part=part: part(core), second[c], when=comes[d]
                )
            share_with(f"{name}{c}{way}{d}", part, when=comes[d])

    for c in range(2):
        net.start(f"a{c}1", lambda c=c: a_own[c](core), first[c])
        go(c, spot(c, z), "b")
    for c in range(2):
        net.start(f"t{c}1", lambda c=c: t_own[c](core), first[c])
        share_with(f"b{c}0", spot(c, z))
        share_with(f"t{c}0", t_own[c])

    def scale(n):
        fetches[n].wait()
        columns = pl.ds(n * side, side)

        def body(i, carry):
            block = pl.ds(pl.multiple_of(i * 128, 128), 128)
            gain = source_gain_ref[:, block].astype(jnp.float32)[n // 2 : n // 2 + 1]
            gain = jnp.transpose(jnp.broadcast_to(gain, (128, 128)))[:, :1]
            weights[block, columns] = (
                weights[block, columns].astype(jnp.float32) * gain
            ).astype(jnp.bfloat16)
            return carry

        lax.fori_loop(0, width // 128, body, 0)

    def own_planes():
        for c in range(2):
            net.arrived(f"a{c}m", lambda: mates(c, z)(core), second[c])
            share_with(f"a{c}m", mates(c, z))
        for c in range(2):
            shared(f"a{c}0", pair(c, z))
            shared(f"a{c}m", mates(c, z))

    def planes_come(d):
        for c in range(2):
            pass_on(c, d, "a", pair)

    def planes_done(d):
        for c in range(2):
            for way, (_, _, began, comes) in ways.items():
                part = mates(c, began[d])
                net.arrived(f"a{c}{way}{d}m", lambda: part(core), second[c], when=comes[d])
                share_with(f"a{c}{way}{d}m", part, when=comes[d])
        for c in range(2):
            for way, (_, _, began, comes) in ways.items():
                shared(f"a{c}{way}{d}", pair(c, began[d]), when=comes[d])
                shared(f"a{c}{way}{d}m", mates(c, began[d]), when=comes[d])

    def rows_done():
        for c in range(2):
            net.arrived(f"t{c}2", lambda: t_two[c](core), second[c])
            share_with(f"t{c}2", t_two[c])

    def columns_come(d):
        for c in range(2):
            pass_on(c, d, "b", spot)

    def columns_go(name, targets):
        for c in range(2):
            part = whole(c, y, x)
            net.start(f"b{c}{name}", lambda part=part: part(core), targets[c])

    def columns_done():
        for c in range(2):
            shared(f"b{c}0", spot(c, z))
            for d in range(1, top + 1):
                for way, (_, _, began, comes) in ways.items():
                    shared(f"b{c}{way}{d}", spot(c, began[d]), when=comes[d])

    def columns_one():
        for c in range(2):
            net.arrived(f"b{c}y", lambda: b_one[c](core), second[c])
            share_with(f"b{c}4", b_one[c])
        for c in range(2):
            shared(f"b{c}4", b_one[c])

    def columns_relay():
        for c in range(2):
            net.start(f"b{c}z", lambda c=c: b_one[c](core), first[c])

    def columns_two():
        for c in range(2):
            net.arrived(f"b{c}x", lambda: b_two[c](core), first[c])
            share_with(f"b{c}5", b_two[c])
        for c in range(2):
            shared(f"b{c}5", b_two[c])

    def columns_last():
        for c in range(2):
            net.arrived(f"b{c}z", lambda: b_last[c](core), first[c])
            share_with(f"b{c}6", b_last[c])
        for c in range(2):
            shared(f"b{c}6", b_last[c])

    scale(0)
    scale(1)
    scale(2)
    for c in range(2):
        net.arrived(f"a{c}1", lambda: a_one[c](core), first[c])
        part = pair(c, z)
        net.start(f"a{c}m", lambda part=part: part(core), second[c])
        share_with(f"a{c}0", part)
    columns_come(1)
    for c in range(2):
        net.arrived(f"t{c}1", lambda: t_one[c](core), first[c])
        net.start(f"t{c}2", lambda c=c: t_have[c](core), second[c])
        share_with(f"t{c}1", t_one[c])
    columns_come(2)
    for c in range(2):
        go(c, pair(c, z), "a")
    scale(3)

    def project_rows(layer, ref):
        rows = normed[layer].reshape(count, width)
        for head in range(group):
            factor = temp_ref[layer, y * group + head] * (HEAD_DIM ** (-0.5) * LOG2E)
            query[head] = (
                jnp.dot(
                    rows,
                    ref[:, head * side : (head + 1) * side],
                    preferred_element_type=jnp.float32,
                )
                * factor
            ).astype(jnp.bfloat16)
        total[...] = jnp.zeros_like(total)
        sums[...] = jnp.zeros_like(sums)
        tops[...] = jnp.full_like(tops, FLOOR)

    def attend(kv):
        keys = kv[:, :, :side].reshape(-1, side)
        values = kv[:, :, side:].reshape(-1, side)
        units = [(head, pl.ds(r, UNIT)) for head in range(group) for r in range(0, count, UNIT)]

        def score(head, block):
            return lax.dot_general(
                query[head, block],
                keys,
                (((1,), (1,)), ((), ())),
                preferred_element_type=jnp.float32,
            )

        ahead = score(*units[0])
        for k, (head, block) in enumerate(units):
            scores = ahead
            if k + 1 < len(units):
                ahead = score(*units[k + 1])
            old_top = tops[head, block, :1]
            new_top = jnp.maximum(old_top, jnp.max(scores, axis=-1, keepdims=True))
            shrink = jnp.exp2(old_top - new_top)
            expo = jnp.exp2(scores - new_top)
            tops[head, block] = jnp.broadcast_to(new_top, (UNIT, tops.shape[2]))
            new_sum = sums[head, block, :1] * shrink + jnp.sum(expo, axis=-1, keepdims=True)
            sums[head, block] = jnp.broadcast_to(new_sum, (UNIT, sums.shape[2]))
            total[head, block] = total[head, block] * shrink + jnp.dot(
                expo.astype(jnp.bfloat16), values, preferred_element_type=jnp.float32
            )

    def first_query():
        rows_done()
        for c in range(2):
            for k, part in enumerate((t_own, t_one, t_two)):
                shared(f"t{c}{k}", part[c])
        finish(query_0)
        project_rows(0, small)
        begin(out_0)

    handlers = {
        0: [own_planes],
        1: [lambda: columns_come(3), lambda: columns_go("y", second), first_query],
        2: [columns_done],
        3: [lambda: planes_come(1)],
        4: [lambda: columns_go("x", first), columns_one],
        6: [lambda: planes_come(2), lambda: planes_done(1)],
        8: [columns_two],
        9: [lambda: planes_come(3), columns_relay],
        10: [lambda: planes_done(2)],
        12: [lambda: planes_done(3)],
        14: [columns_last],
    }
    low = z < 2
    near = jnp.where(z == 0, 1, jnp.where(z == 1, 0, jnp.where(z == 2, 3, 2)))
    next_one = jnp.where(low, 2, 1)
    far = jnp.where(low, 3, 0)
    order = [
        z, 4 + z, 8 + y * 2 + x, 12 + y * 2 + x,
        8 + me.oy * 2 + x, 12 + y * 2 + me.ox, near, 4 + near,
        8 + y * 2 + me.ox, 12 + me.oy * 2 + x, next_one, 4 + next_one,
        far, 4 + far, 8 + me.oy * 2 + me.ox, 12 + me.oy * 2 + me.ox,
    ]

    kept = steps - LATER

    def block_at(s):
        which = order[0]
        for k in range(1, steps):
            which = jnp.where(s == k, order[k], which)
        return blocks[which].reshape(positions, width)

    def made(block, n):
        return jnp.dot(
            block, weights[:, n * side : (n + 1) * side], preferred_element_type=jnp.float32
        ).astype(jnp.bfloat16)

    def project_late(s, carry=0):
        block = block_at(s)
        for n in range(2):
            late[s, :, n * side : (n + 1) * side] = made(block, 2 + n)
        return carry

    def step(s, carry):
        for k, calls in handlers.items():

            @pl.when(s == k)
            def _():
                for call in calls:
                    call()

        block = block_at(s)
        for n in range(2):
            early[s % 2, :, n * side : (n + 1) * side] = made(block, n)

        @pl.when(s < kept)
        def _():
            project_late(s)

        @pl.when(s % 2 == 1)
        def _():
            attend(early)

        return carry

    lax.fori_loop(0, steps, step, 0)
    begin(query_1)
    waits = iter(range(4))

    def meanwhile():
        k, each = next(waits), LATER // 4
        lax.fori_loop(kept + k * each, kept + (k + 1) * each, project_late, 0)

    def out_rows(layer, ref, c):
        block = slice(c * (count // 2), (c + 1) * (count // 2))
        attended = jnp.concatenate(
            [
                (total[head, block] / sums[head, block, :1]).astype(jnp.bfloat16)
                for head in range(group)
            ],
            axis=1,
        )
        half = width // 2
        for k in range(2):
            for n in range(0, half, side):
                term = jnp.dot(
                    attended,
                    ref[k * half : (k + 1) * half, n : n + side],
                    preferred_element_type=jnp.float32,
                ).astype(jnp.bfloat16)
                partial[c, :, :, :, :, k * half + n : k * half + n + side] = term.reshape(
                    2, 2, 2, share, side
                )

    sides = [[me.oy, y], [me.ox, x]]
    spots = [(x, me.ox), (y, me.oy)]

    def piece_of(c, k, who):
        return partial.at[c, sides[c][k], :, who] if c == 0 else partial.at[c, :, sides[c][k], who]

    def fold_start(layer, c):
        for k in range(2):
            net.start(
                f"c{c}{k}{layer}",
                lambda c=c, k=k: piece_of(c, k, me.other),
                sibling,
                lambda c=c, k=k: from_core.at[layer, c, k],
            )

    def fold_pairs(layer, between=lambda: None):
        for k in range(2):
            for c in range(2):
                net.arrived(f"c{c}{k}{layer}", lambda: from_core.at[layer, c, k], sibling)
                pieces[c, k] = (
                    piece_of(c, k, core)[...].astype(jnp.float32)
                    + from_core[layer, c, k].astype(jnp.float32)
                ).astype(jnp.bfloat16)
                if k == 0:
                    net.start(
                        f"p{c}{layer}",
                        lambda c=c: pieces.at[c, 0],
                        second[c],
                        lambda c=c: from_first.at[layer, c],
                    )
        between()
        for c in range(2):
            far = spots[c][1]
            net.arrived(f"p{c}{layer}", lambda: from_first.at[layer, c], second[c])
            relay[c] = (
                pieces[c, 1, far].astype(jnp.float32) + from_first[layer, c, far].astype(jnp.float32)
            ).astype(jnp.bfloat16)
            net.start(
                f"q{c}{layer}",
                lambda c=c: relay.at[c],
                first[c],
                lambda c=c: from_second.at[layer, c],
            )

    def folded(layer, c):
        near = spots[c][0]
        partly = pieces[c, 1, near].astype(jnp.float32) + from_first[layer, c, near].astype(
            jnp.float32
        )
        net.arrived(f"q{c}{layer}", lambda: from_second.at[layer, c], first[c])
        return state[c] + (partly + from_second[layer, c].astype(jnp.float32))

    finish(out_0)
    for c in range(2):
        out_rows(0, small, c)
        fold_start(0, c)
    fold_pairs(0, meanwhile)
    meanwhile()
    own = [lambda k, c=c: normed.at[1, c, y, x, k] for c in range(2)]
    one = [lambda k: normed.at[1, 0, y, me.ox, k], lambda k: normed.at[1, 1, me.oy, x, k]]
    two = [lambda k: normed.at[1, 0, me.oy, :, k], lambda k: normed.at[1, 1, :, me.ox, k]]
    have = [lambda k: normed.at[1, 0, y, :, k], lambda k: normed.at[1, 1, :, x, k]]
    for c in range(2):
        rows = folded(0, c)
        state[c] = rows
        normed[1, c, y, x, core] = (unit_rows(rows) * target_gain[1:2]).astype(jnp.bfloat16)
        net.start(f"n{c}1", lambda c=c: own[c](core), first[c])
        share_with(f"n{c}0", own[c])
    meanwhile()
    for c in range(2):
        net.arrived(f"n{c}1", lambda: one[c](core), first[c])
        net.start(f"n{c}2", lambda c=c: have[c](core), second[c])
        share_with(f"n{c}1", one[c])
    meanwhile()
    begin(out_1)
    for c in range(2):
        net.arrived(f"n{c}2", lambda: two[c](core), second[c])
        share_with(f"n{c}2", two[c])
    for c in range(2):
        for k, part in enumerate((own, one, two)):
            shared(f"n{c}{k}", part[c])
    net.drain()
    finish(query_1)
    project_rows(1, late_query)

    def second_step(j, carry):
        attend(late.at[pl.ds(4 * j, 4)])
        return carry

    lax.fori_loop(0, steps // 4, second_step, 0)
    finish(out_1)
    for c in range(2):
        out_rows(1, late_out, c)
        fold_start(1, c)
    fold_pairs(1)
    for c in range(2):
        rows = unit_rows(folded(1, c)) * final_gain_ref[...].astype(jnp.float32)
        result_ref[c * share : (c + 1) * share] = rows
    net.drain()


def on_planes(
    target, source, target_gain, source_gain, query_w, key_w, value_w, out_w, head_temp, final_gain
):
    width = target.shape[1]
    group = query_w.shape[2] // key_w.shape[2]
    piece, share = source.shape[0] // 4, target.shape[0] // 2
    count, positions, copies = 16 * share, 8 * piece, 140
    part = (2, share, width)
    return pl.pallas_call(
        functools.partial(whole_kernel, group),
        out_shape=jax.ShapeDtypeStruct(target.shape, jnp.float32),
        in_specs=[VMEM, VMEM, HBM, HBM, HBM, HBM, VMEM, VMEM, VMEM, SMEM],
        out_specs=VMEM,
        scratch_shapes=[
            pltpu.VMEM((16, 2, 2, 2, piece, width), jnp.bfloat16),
            pltpu.VMEM((2, 2, 2, 2, 2, share, width), jnp.bfloat16),
            pltpu.VMEM((width, 4 * HEAD_DIM), jnp.bfloat16),
            pltpu.VMEM((width, group * HEAD_DIM), jnp.bfloat16),
            pltpu.VMEM((2, positions, 2 * HEAD_DIM), jnp.bfloat16),
            pltpu.VMEM((16, positions, 2 * HEAD_DIM), jnp.bfloat16),
            pltpu.VMEM((group, count, HEAD_DIM), jnp.bfloat16),
            pltpu.VMEM((group, count, HEAD_DIM), jnp.float32),
            pltpu.VMEM((group, count, 128), jnp.float32),
            pltpu.VMEM((group, count, 128), jnp.float32),
            pltpu.VMEM((2, 2, 2, 2, share, width), jnp.bfloat16),
            pltpu.VMEM((2, 2, 2, share, width), jnp.bfloat16),
            pltpu.VMEM((2, 2, 2, 2, share, width), jnp.bfloat16),
            pltpu.VMEM((2, 2, 2, share, width), jnp.bfloat16),
            pltpu.VMEM((2, 2, share, width), jnp.bfloat16),
            pltpu.VMEM((2, share, width), jnp.bfloat16),
            pltpu.VMEM(part, jnp.float32),
            pltpu.SemaphoreType.DMA((copies,)),
            pltpu.SemaphoreType.DMA((copies,)),
            pltpu.SemaphoreType.DMA((10,)),
        ],
        compiler_params=pltpu.CompilerParams(
            collective_id=0, has_side_effects=True, vmem_limit_bytes=63 * MIB
        ),
    )(
        source,
        target,
        key_w,
        value_w,
        query_w,
        out_w,
        source_gain,
        target_gain,
        final_gain.reshape(1, width),
        head_temp,
    )


def shifted(block, shift):
    size = lax.axis_size("tp")
    return lax.ppermute(block, "tp", [(i, (i + shift) % size) for i in range(size)])


def gather_rows(block):
    size = lax.axis_size("tp")
    return jnp.concatenate([block] + [shifted(block, k) for k in range(1, size)], axis=0)


def return_rows(blocks):
    size = lax.axis_size("tp")
    count = blocks.shape[0] // size
    mixed = blocks[:count].astype(jnp.float32)
    for k in range(1, size):
        mixed += shifted(blocks[k * count : (k + 1) * count], -k).astype(jnp.float32)
    return mixed


def flash_kernel(rows, query_ref, source_ref, mix_ref, total_ref, top_ref, sum_ref):
    step = pl.program_id(0)
    count = query_ref.shape[0]

    @pl.when(step == 0)
    def _():
        total_ref[...] = jnp.zeros_like(total_ref)
        sum_ref[...] = jnp.zeros_like(sum_ref)
        top_ref[...] = jnp.full_like(top_ref, FLOOR)

    for start in range(0, count, rows):
        block = pl.ds(start, rows)
        scores = lax.dot_general(
            query_ref[block, :],
            source_ref[...],
            (((1,), (1,)), ((), ())),
            preferred_element_type=jnp.float32,
        )
        old_top = top_ref[block, :1]
        new_top = jnp.maximum(old_top, jnp.max(scores, axis=-1, keepdims=True))
        shrink = jnp.exp2(old_top - new_top)
        expo = jnp.exp2(scores - new_top)
        top_ref[block, :] = jnp.broadcast_to(new_top, (rows, top_ref.shape[1]))
        new_sum = sum_ref[block, :1] * shrink + jnp.sum(expo, axis=-1, keepdims=True)
        sum_ref[block, :] = jnp.broadcast_to(new_sum, (rows, sum_ref.shape[1]))
        total_ref[block, :] = total_ref[block, :] * shrink + jnp.dot(
            expo.astype(jnp.bfloat16), source_ref[...], preferred_element_type=jnp.float32
        )

    @pl.when(step == pl.num_programs(0) - 1)
    def _():
        for start in range(0, count, rows):
            block = pl.ds(start, rows)
            mix_ref[block, :] = (total_ref[block, :] / sum_ref[block, :1]).astype(mix_ref.dtype)


def attend(query, source, chunk=CHUNK, rows=ROWS):
    count, width = query.shape
    positions = source.shape[0]
    chunk = math.gcd(chunk, positions)
    rows = math.gcd(rows, count)
    return pl.pallas_call(
        functools.partial(flash_kernel, rows),
        grid=(positions // chunk,),
        out_shape=jax.ShapeDtypeStruct((count, width), jnp.bfloat16),
        in_specs=[
            pl.BlockSpec((count, width), lambda j: (0, 0), pipeline_mode=pl.Buffered(1)),
            pl.BlockSpec((chunk, width), lambda j: (j, 0)),
        ],
        out_specs=pl.BlockSpec((count, width), lambda j: (0, 0), pipeline_mode=pl.Buffered(1)),
        scratch_shapes=[
            pltpu.VMEM((count, width), jnp.float32),
            pltpu.VMEM((count, 128), jnp.float32),
            pltpu.VMEM((count, 128), jnp.float32),
        ],
        compiler_params=pltpu.CompilerParams(
            dimension_semantics=("arbitrary",), vmem_limit_bytes=56 * 1024 * 1024
        ),
        cost_estimate=pl.CostEstimate(
            flops=4 * count * positions * width,
            bytes_accessed=2 * positions * width,
            transcendentals=count * positions,
        ),
    )(query, source)


def per_device(
    target, source, target_gain, source_gain, query_w, key_w, value_w, out_w, head_temp, final_gain
):
    width = target.shape[1]
    heads = query_w.shape[2] // HEAD_DIM
    shared = key_w.shape[2] // HEAD_DIM
    group = heads // shared
    positions = lax.all_gather(
        unit_rows(source).astype(jnp.bfloat16), ("sp", "tp"), axis=0, tiled=True
    )
    hidden_state = target.astype(jnp.float32)
    for layer in range(2):
        gain = source_gain[layer].astype(jnp.float32)
        normed = (unit_rows(hidden_state) * target_gain[layer].astype(jnp.float32)).astype(
            jnp.bfloat16
        )
        queries = jnp.dot(
            gather_rows(normed),
            query_w[layer],
            preferred_element_type=jnp.float32,
        ).astype(jnp.bfloat16)
        count = queries.shape[0]
        scales = head_temp[layer] * (HEAD_DIM ** (-0.5) * LOG2E)
        lifted = []
        for head in range(heads):
            columns = slice((head // group) * HEAD_DIM, (head // group + 1) * HEAD_DIM)
            lifted.append(
                (
                    lax.dot_general(
                        queries[:, head * HEAD_DIM : (head + 1) * HEAD_DIM],
                        key_w[layer][:, columns],
                        (((1,), (1,)), ((), ())),
                        preferred_element_type=jnp.float32,
                    )
                    * (gain * scales[head])
                ).astype(jnp.bfloat16)
            )
        mix = attend(jnp.concatenate(lifted, axis=0), positions)
        attended = []
        for head in range(heads):
            columns = slice((head // group) * HEAD_DIM, (head // group + 1) * HEAD_DIM)
            own = (mix[head * count : (head + 1) * count].astype(jnp.float32) * gain).astype(
                jnp.bfloat16
            )
            attended.append(
                jnp.dot(
                    own, value_w[layer][:, columns], preferred_element_type=jnp.float32
                ).astype(jnp.bfloat16)
            )
        mixed = return_rows(
            jnp.dot(
                jnp.concatenate(attended, axis=1),
                out_w[layer],
                preferred_element_type=jnp.float32,
            ).astype(jnp.bfloat16)
        )
        hidden_state = hidden_state + mixed
    return unit_rows(hidden_state) * final_gain.astype(jnp.float32)


def fits(mesh):
    return dict(mesh.shape) == {"sp": 8, "tp": 4}


def solution(mesh):
    in_specs = (
        P(("sp", "tp"), None),
        P(("sp", "tp"), None),
        P(),
        P(),
        P(None, None, "tp"),
        P(None, None, "tp"),
        P(None, None, "tp"),
        P(None, "tp", None),
        P(None, "tp"),
        P(),
    )
    out_specs = P(("sp", "tp"), None)
    return jax.shard_map(
        on_planes if fits(mesh) else per_device, mesh=mesh, in_specs=in_specs, out_specs=out_specs, check_vma=False
    )
```

```python
import functools
import math

import jax
import jax.numpy as jnp
from jax import lax
from jax.experimental import pallas as pl
from jax.experimental.pallas import tpu as pltpu
from jax.sharding import PartitionSpec as P

HEAD_DIM = 512
EPS = 1e-06
FLOOR = -1e30
CHUNK = 512
ROWS = 512
UNIT = 256
LOG2E = math.log2(math.e)
LATER = 12
MESH = pl.DeviceIdType.MESH
MIB = 1024 * 1024
HBM = pl.BlockSpec(memory_space=pl.ANY)
VMEM = pl.BlockSpec(memory_space=pltpu.VMEM)
SMEM = pl.BlockSpec(memory_space=pltpu.SMEM)


def unit_rows(matrix):
    values = matrix.astype(jnp.float32)
    return values * lax.rsqrt(jnp.mean(values * values, axis=-1, keepdims=True) + EPS)


class Place:
    def __init__(self):
        sp, tp = lax.axis_index("sp"), lax.axis_index("tp")
        self.z, self.y = sp // 2, sp % 2
        self.x, self.core = tp // 2, tp % 2
        self.up, self.down = (self.z + 1) % 4, (self.z + 3) % 4
        self.far = (self.z + 2) % 4
        self.ox, self.oy, self.other = 1 - self.x, 1 - self.y, 1 - self.core

    def at(self, z=None, y=None, x=None, core=None):
        z = self.z if z is None else z
        y = self.y if y is None else y
        x = self.x if x is None else x
        core = self.core if core is None else core
        return (z * 2 + y, x * 2 + core)


class Copies:
    def __init__(self, send_sems, recv_sems):
        self.send_sems, self.recv_sems = send_sems, recv_sems
        self.index, self.sent = {}, []

    def _make(self, name, ref, target, dst=None):
        k = self.index.setdefault(name, len(self.index))
        return pltpu.make_async_remote_copy(
            src_ref=ref,
            dst_ref=ref if dst is None else dst,
            send_sem=self.send_sems.at[k],
            recv_sem=self.recv_sems.at[k],
            device_id=target,
            device_id_type=MESH,
        )

    def start(self, name, src, target, dst=None, when=None):
        self.sent.append((name, src, target, dst, when))
        perhaps(when, lambda: self._make(name, src(), target, dst and dst()).start())

    def arrived(self, name, ref, source, when=None):
        perhaps(when, lambda: self._make(name, ref(), source).wait_recv())

    def drain(self):
        for name, src, target, dst, when in self.sent:
            perhaps(when, lambda: self._make(name, src(), target, dst and dst()).wait_send())
        self.sent = []


def perhaps(when, call):
    if when is None:
        call()
    else:
        pl.when(when)(call)


def greet(targets):
    barrier = pltpu.get_barrier_semaphore()
    for target in targets:
        pl.semaphore_signal(barrier, inc=1, device_id=target, device_id_type=MESH)
    return lambda: pl.semaphore_wait(barrier, len(targets))


def whole_kernel(
    group, source_ref, target_ref, key_ref, value_ref, query_ref, out_ref, source_gain_ref,
    target_gain_ref, final_gain_ref, temp_ref,
    result_ref,
    blocks, normed, weights, small, early, late, query, total, tops, sums, partial, pieces,
    from_core, from_first, from_second, relay, state,
    send_sems, recv_sems, weight_sems,
):
    me = Place()
    z, y, x, core = me.z, me.y, me.x, me.core
    width = weights.shape[0]
    side, wide = HEAD_DIM, group * HEAD_DIM
    steps, positions = blocks.shape[0], math.prod(blocks.shape[1:5])
    share, piece = normed.shape[5], blocks.shape[4]
    count = 16 * share
    span = pl.ds(pl.multiple_of(y * wide, wide), wide)

    def plane(c, zz):
        return blocks.at[c * 4 + zz]

    def column(c, yy, xx):
        return blocks.at[8 + c * 4 + yy * 2 + xx]

    fetches = []
    for layer in range(2):
        for part, ref in enumerate((key_ref, value_ref)):
            n = 2 * layer + part
            fetches.append(
                pltpu.make_async_copy(
                    ref.at[layer, :, pl.ds(pl.multiple_of(y * side, side), side)],
                    weights.at[:, pl.ds(n * side, side)],
                    weight_sems.at[n],
                )
            )

    def query_fetch(layer, dst, sem):
        return [pltpu.make_async_copy(query_ref.at[layer, :, span], dst, weight_sems.at[sem])]

    def out_fetch(layer, dst, sem):
        half = width // 2
        return [
            pltpu.make_async_copy(
                out_ref.at[layer, span, pl.ds(k * half, half)],
                dst.at[pl.ds(k * half, half)],
                weight_sems.at[sem + k],
            )
            for k in range(2)
        ]

    late_query, late_out = weights.at[:, pl.ds(0, wide)], weights.at[:, pl.ds(wide, wide)]
    query_0, out_0 = query_fetch(0, small, 4), out_fetch(0, small, 5)
    query_1, out_1 = query_fetch(1, late_query, 7), out_fetch(1, late_out, 8)

    def begin(copies):
        for copy in copies:
            copy.start()

    def finish(copies):
        for copy in copies:
            copy.wait()

    target_gain = target_gain_ref[...].astype(jnp.float32)
    all_here = greet([me.at(x=me.ox), me.at(y=me.oy), me.at(z=me.up), me.at(z=me.down), me.at(core=me.other)])
    begin(fetches)
    begin(query_0)
    for c in range(2):
        of_plane = source_ref[c * piece : (c + 1) * piece]
        of_column = source_ref[(2 + c) * piece : (3 + c) * piece]
        blocks[c * 4 + z, y, x, core] = unit_rows(of_plane).astype(jnp.bfloat16)
        blocks[8 + c * 4 + y * 2 + x, z // 2, z % 2, core] = unit_rows(of_column).astype(
            jnp.bfloat16
        )
        rows = target_ref[c * share : (c + 1) * share].astype(jnp.float32)
        state[c] = rows
        normed[0, c, y, x, core] = (unit_rows(rows) * target_gain[0:1]).astype(jnp.bfloat16)
    all_here()

    net = Copies(send_sems, recv_sems)
    sibling, xmate, ymate = me.at(core=me.other), me.at(x=me.ox), me.at(y=me.oy)
    above, below = me.at(z=me.up), me.at(z=me.down)
    first, second = [xmate, ymate], [ymate, xmate]

    def share_with(name, part, when=None):
        net.start(name + "d", lambda: part(core), sibling, when=when)

    def shared(name, part, when=None):
        net.arrived(name + "d", lambda: part(me.other), sibling, when=when)

    def pair(c, zz):
        return lambda k: plane(c, zz).at[y, :, k] if c == 0 else plane(c, zz).at[:, x, k]

    def mates(c, zz):
        return lambda k: plane(c, zz).at[me.oy, :, k] if c == 0 else plane(c, zz).at[:, me.ox, k]

    def spot(c, zz):
        return lambda k: column(c, y, x).at[zz // 2, zz % 2, k]

    def whole(c, yy, xx):
        return lambda k: column(c, yy, xx).at[:, :, k]

    a_own = [lambda k, c=c: plane(c, z).at[y, x, k] for c in range(2)]
    a_one = [lambda k: plane(0, z).at[y, me.ox, k], lambda k: plane(1, z).at[me.oy, x, k]]
    b_one = [whole(0, me.oy, x), whole(1, y, me.ox)]
    b_two = [whole(0, y, me.ox), whole(1, me.oy, x)]
    b_last = [whole(c, me.oy, me.ox) for c in range(2)]
    t_own = [lambda k, c=c: normed.at[0, c, y, x, k] for c in range(2)]
    t_one = [lambda k: normed.at[0, 0, y, me.ox, k], lambda k: normed.at[0, 1, me.oy, x, k]]
    t_two = [lambda k: normed.at[0, 0, me.oy, :, k], lambda k: normed.at[0, 1, :, me.ox, k]]
    t_have = [lambda k: normed.at[0, 0, y, :, k], lambda k: normed.at[0, 1, :, x, k]]
    top = 3
    hops = range(top + 1)
    ways = {
        "u": (below, above, [z - d for d in hops], [z >= d for d in hops]),
        "w": (above, below, [z + d for d in hops], [z + d <= top for d in hops]),
    }
    more = {"u": z < top, "w": z > 0}
    goes = {way: [jnp.logical_and(c, more[way]) for c in ways[way][3]] for way in ways}

    def go(c, part, name):
        for way, (_, ahead, _, _) in ways.items():
            net.start(f"{name}{c}{way}1", lambda: part(core), ahead, when=more[way])

    def pass_on(c, d, name, region):
        for way, (behind, ahead, began, comes) in ways.items():
            part = region(c, began[d])
            net.arrived(f"{name}{c}{way}{d}", lambda: part(core), behind, when=comes[d])
            if d < top:
                net.start(
                    f"{name}{c}{way}{d + 1}",
                    lambda part=part: part(core),
                    ahead,
                    when=goes[way][d],
                )
            if name == "a":
                net.start(
                    f"a{c}{way}{d}m", lambda part=part: part(core), second[c], when=comes[d]
                )
            share_with(f"{name}{c}{way}{d}", part, when=comes[d])

    for c in range(2):
        net.start(f"a{c}1", lambda c=c: a_own[c](core), first[c])
        go(c, spot(c, z), "b")
    for c in range(2):
        net.start(f"t{c}1", lambda c=c: t_own[c](core), first[c])
        share_with(f"b{c}0", spot(c, z))
        share_with(f"t{c}0", t_own[c])

    def scale(n):
        fetches[n].wait()
        columns = pl.ds(n * side, side)

        def body(i, carry):
            block = pl.ds(pl.multiple_of(i * 128, 128), 128)
            gain = source_gain_ref[:, block].astype(jnp.float32)[n // 2 : n // 2 + 1]
            gain = jnp.transpose(jnp.broadcast_to(gain, (128, 128)))[:, :1]
            weights[block, columns] = (
                weights[block, columns].astype(jnp.float32) * gain
            ).astype(jnp.bfloat16)
            return carry

        lax.fori_loop(0, width // 128, body, 0)

    def own_planes():
        for c in range(2):
            net.arrived(f"a{c}m", lambda: mates(c, z)(core), second[c])
            share_with(f"a{c}m", mates(c, z))
        for c in range(2):
            shared(f"a{c}0", pair(c, z))
            shared(f"a{c}m", mates(c, z))

    def planes_come(d):
        for c in range(2):
            pass_on(c, d, "a", pair)

    def planes_done(d):
        for c in range(2):
            for way, (_, _, began, comes) in ways.items():
                part = mates(c, began[d])
                net.arrived(f"a{c}{way}{d}m", lambda: part(core), second[c], when=comes[d])
                share_with(f"a{c}{way}{d}m", part, when=comes[d])
        for c in range(2):
            for way, (_, _, began, comes) in ways.items():
                shared(f"a{c}{way}{d}", pair(c, began[d]), when=comes[d])
                shared(f"a{c}{way}{d}m", mates(c, began[d]), when=comes[d])

    def rows_done():
        for c in range(2):
            net.arrived(f"t{c}2", lambda: t_two[c](core), second[c])
            share_with(f"t{c}2", t_two[c])

    def columns_come(d):
        for c in range(2):
            pass_on(c, d, "b", spot)

    def columns_go(name, targets):
        for c in range(2):
            part = whole(c, y, x)
            net.start(f"b{c}{name}", lambda part=part: part(core), targets[c])

    def columns_done():
        for c in range(2):
            shared(f"b{c}0", spot(c, z))
            for d in range(1, top + 1):
                for way, (_, _, began, comes) in ways.items():
                    shared(f"b{c}{way}{d}", spot(c, began[d]), when=comes[d])

    def columns_one():
        for c in range(2):
            net.arrived(f"b{c}y", lambda: b_one[c](core), second[c])
            share_with(f"b{c}4", b_one[c])
        for c in range(2):
            shared(f"b{c}4", b_one[c])

    def columns_relay():
        for c in range(2):
            net.start(f"b{c}z", lambda c=c: b_one[c](core), first[c])

    def columns_two():
        for c in range(2):
            net.arrived(f"b{c}x", lambda: b_two[c](core), first[c])
            share_with(f"b{c}5", b_two[c])
        for c in range(2):
            shared(f"b{c}5", b_two[c])

    def columns_last():
        for c in range(2):
            net.arrived(f"b{c}z", lambda: b_last[c](core), first[c])
            share_with(f"b{c}6", b_last[c])
        for c in range(2):
            shared(f"b{c}6", b_last[c])

    scale(0)
    scale(1)
    scale(2)
    for c in range(2):
        net.arrived(f"a{c}1", lambda: a_one[c](core), first[c])
        part = pair(c, z)
        net.start(f"a{c}m", lambda part=part: part(core), second[c])
        share_with(f"a{c}0", part)
    columns_come(1)
    for c in range(2):
        net.arrived(f"t{c}1", lambda: t_one[c](core), first[c])
        net.start(f"t{c}2", lambda c=c: t_have[c](core), second[c])
        share_with(f"t{c}1", t_one[c])
    columns_come(2)
    for c in range(2):
        go(c, pair(c, z), "a")
    scale(3)

    def project_rows(layer, ref):
        rows = normed[layer].reshape(count, width)
        for head in range(group):
            factor = temp_ref[layer, y * group + head] * (HEAD_DIM ** (-0.5) * LOG2E)
            query[head] = (
                jnp.dot(
                    rows,
                    ref[:, head * side : (head + 1) * side],
                    preferred_element_type=jnp.float32,
                )
                * factor
            ).astype(jnp.bfloat16)
        total[...] = jnp.zeros_like(total)
        sums[...] = jnp.zeros_like(sums)
        tops[...] = jnp.full_like(tops, FLOOR)

    def attend(kv):
        keys = kv[:, :, :side].reshape(-1, side)
        values = kv[:, :, side:].reshape(-1, side)
        units = [(head, pl.ds(r, UNIT)) for head in range(group) for r in range(0, count, UNIT)]

        def score(head, block):
            return lax.dot_general(
                query[head, block],
                keys,
                (((1,), (1,)), ((), ())),
                preferred_element_type=jnp.float32,
            )

        ahead = score(*units[0])
        for k, (head, block) in enumerate(units):
            scores = ahead
            if k + 1 < len(units):
                ahead = score(*units[k + 1])
            old_top = tops[head, block, :1]
            new_top = jnp.maximum(old_top, jnp.max(scores, axis=-1, keepdims=True))
            shrink = jnp.exp2(old_top - new_top)
            expo = jnp.exp2(scores - new_top)
            tops[head, block] = jnp.broadcast_to(new_top, (UNIT, tops.shape[2]))
            new_sum = sums[head, block, :1] * shrink + jnp.sum(expo, axis=-1, keepdims=True)
            sums[head, block] = jnp.broadcast_to(new_sum, (UNIT, sums.shape[2]))
            total[head, block] = total[head, block] * shrink + jnp.dot(
                expo.astype(jnp.bfloat16), values, preferred_element_type=jnp.float32
            )

    def first_query():
        rows_done()
        for c in range(2):
            for k, part in enumerate((t_own, t_one, t_two)):
                shared(f"t{c}{k}", part[c])
        finish(query_0)
        project_rows(0, small)
        begin(out_0)

    handlers = {
        0: [own_planes],
        1: [lambda: columns_come(3), lambda: columns_go("y", second), first_query],
        2: [columns_done],
        3: [lambda: planes_come(1)],
        4: [lambda: columns_go("x", first), columns_one],
        6: [lambda: planes_come(2), lambda: planes_done(1)],
        8: [columns_two],
        9: [lambda: planes_come(3), columns_relay],
        10: [lambda: planes_done(2)],
        12: [lambda: planes_done(3)],
        14: [columns_last],
    }
    low = z < 2
    near = jnp.where(z == 0, 1, jnp.where(z == 1, 0, jnp.where(z == 2, 3, 2)))
    next_one = jnp.where(low, 2, 1)
    far = jnp.where(low, 3, 0)
    order = [
        z, 4 + z, 8 + y * 2 + x, 12 + y * 2 + x,
        8 + me.oy * 2 + x, 12 + y * 2 + me.ox, near, 4 + near,
        8 + y * 2 + me.ox, 12 + me.oy * 2 + x, next_one, 4 + next_one,
        far, 4 + far, 8 + me.oy * 2 + me.ox, 12 + me.oy * 2 + me.ox,
    ]

    kept = steps - LATER

    def block_at(s):
        which = order[0]
        for k in range(1, steps):
            which = jnp.where(s == k, order[k], which)
        return blocks[which].reshape(positions, width)

    def made(block, n):
        return jnp.dot(
            block, weights[:, n * side : (n + 1) * side], preferred_element_type=jnp.float32
        ).astype(jnp.bfloat16)

    def project_late(s, carry=0):
        block = block_at(s)
        for n in range(2):
            late[s, :, n * side : (n + 1) * side] = made(block, 2 + n)
        return carry

    def step(s, carry):
        for k, calls in handlers.items():

            @pl.when(s == k)
            def _():
                for call in calls:
                    call()

        block = block_at(s)
        for n in range(2):
            early[s % 2, :, n * side : (n + 1) * side] = made(block, n)

        @pl.when(s < kept)
        def _():
            project_late(s)

        @pl.when(s % 2 == 1)
        def _():
            attend(early)

        return carry

    lax.fori_loop(0, steps, step, 0)
    begin(query_1)
    waits = iter(range(4))

    def meanwhile():
        k, each = next(waits), LATER // 4
        lax.fori_loop(kept + k * each, kept + (k + 1) * each, project_late, 0)

    def out_rows(layer, ref, c):
        block = slice(c * (count // 2), (c + 1) * (count // 2))
        attended = jnp.concatenate(
            [
                (total[head, block] / sums[head, block, :1]).astype(jnp.bfloat16)
                for head in range(group)
            ],
            axis=1,
        )
        half = width // 2
        for k in range(2):
            for n in range(0, half, side):
                term = jnp.dot(
                    attended,
                    ref[k * half : (k + 1) * half, n : n + side],
                    preferred_element_type=jnp.float32,
                ).astype(jnp.bfloat16)
                partial[c, :, :, :, :, k * half + n : k * half + n + side] = term.reshape(
                    2, 2, 2, share, side
                )

    sides = [[me.oy, y], [me.ox, x]]
    spots = [(x, me.ox), (y, me.oy)]

    def piece_of(c, k, who):
        return partial.at[c, sides[c][k], :, who] if c == 0 else partial.at[c, :, sides[c][k], who]

    def fold_start(layer, c):
        for k in range(2):
            net.start(
                f"c{c}{k}{layer}",
                lambda c=c, k=k: piece_of(c, k, me.other),
                sibling,
                lambda c=c, k=k: from_core.at[layer, c, k],
            )

    def fold_pairs(layer, between=lambda: None):
        for k in range(2):
            for c in range(2):
                net.arrived(f"c{c}{k}{layer}", lambda: from_core.at[layer, c, k], sibling)
                pieces[c, k] = (
                    piece_of(c, k, core)[...].astype(jnp.float32)
                    + from_core[layer, c, k].astype(jnp.float32)
                ).astype(jnp.bfloat16)
                if k == 0:
                    net.start(
                        f"p{c}{layer}",
                        lambda c=c: pieces.at[c, 0],
                        second[c],
                        lambda c=c: from_first.at[layer, c],
                    )
        between()
        for c in range(2):
            far = spots[c][1]
            net.arrived(f"p{c}{layer}", lambda: from_first.at[layer, c], second[c])
            relay[c] = (
                pieces[c, 1, far].astype(jnp.float32) + from_first[layer, c, far].astype(jnp.float32)
            ).astype(jnp.bfloat16)
            net.start(
                f"q{c}{layer}",
                lambda c=c: relay.at[c],
                first[c],
                lambda c=c: from_second.at[layer, c],
            )

    def folded(layer, c):
        near = spots[c][0]
        partly = pieces[c, 1, near].astype(jnp.float32) + from_first[layer, c, near].astype(
            jnp.float32
        )
        net.arrived(f"q{c}{layer}", lambda: from_second.at[layer, c], first[c])
        return state[c] + (partly + from_second[layer, c].astype(jnp.float32))

    finish(out_0)
    for c in range(2):
        out_rows(0, small, c)
        fold_start(0, c)
    fold_pairs(0, meanwhile)
    meanwhile()
    own = [lambda k, c=c: normed.at[1, c, y, x, k] for c in range(2)]
    one = [lambda k: normed.at[1, 0, y, me.ox, k], lambda k: normed.at[1, 1, me.oy, x, k]]
    two = [lambda k: normed.at[1, 0, me.oy, :, k], lambda k: normed.at[1, 1, :, me.ox, k]]
    have = [lambda k: normed.at[1, 0, y, :, k], lambda k: normed.at[1, 1, :, x, k]]
    for c in range(2):
        rows = folded(0, c)
        state[c] = rows
        normed[1, c, y, x, core] = (unit_rows(rows) * target_gain[1:2]).astype(jnp.bfloat16)
        net.start(f"n{c}1", lambda c=c: own[c](core), first[c])
        share_with(f"n{c}0", own[c])
    meanwhile()
    for c in range(2):
        net.arrived(f"n{c}1", lambda: one[c](core), first[c])
        net.start(f"n{c}2", lambda c=c: have[c](core), second[c])
        share_with(f"n{c}1", one[c])
    meanwhile()
    begin(out_1)
    for c in range(2):
        net.arrived(f"n{c}2", lambda: two[c](core), second[c])
        share_with(f"n{c}2", two[c])
    for c in range(2):
        for k, part in enumerate((own, one, two)):
            shared(f"n{c}{k}", part[c])
    net.drain()
    finish(query_1)
    project_rows(1, late_query)

    def second_step(j, carry):
        attend(late.at[pl.ds(4 * j, 4)])
        return carry

    lax.fori_loop(0, steps // 4, second_step, 0)
    finish(out_1)
    for c in range(2):
        out_rows(1, late_out, c)
        fold_start(1, c)
    fold_pairs(1)
    for c in range(2):
        rows = unit_rows(folded(1, c)) * final_gain_ref[...].astype(jnp.float32)
        result_ref[c * share : (c + 1) * share] = rows
    net.drain()


def on_planes(
    target, source, target_gain, source_gain, query_w, key_w, value_w, out_w, head_temp, final_gain
):
    width = target.shape[1]
    group = query_w.shape[2] // key_w.shape[2]
    piece, share = source.shape[0] // 4, target.shape[0] // 2
    count, positions, copies = 16 * share, 8 * piece, 140
    part = (2, share, width)
    return pl.pallas_call(
        functools.partial(whole_kernel, group),
        out_shape=jax.ShapeDtypeStruct(target.shape, jnp.float32),
        in_specs=[VMEM, VMEM, HBM, HBM, HBM, HBM, VMEM, VMEM, VMEM, SMEM],
        out_specs=VMEM,
        scratch_shapes=[
            pltpu.VMEM((16, 2, 2, 2, piece, width), jnp.bfloat16),
            pltpu.VMEM((2, 2, 2, 2, 2, share, width), jnp.bfloat16),
            pltpu.VMEM((width, 4 * HEAD_DIM), jnp.bfloat16),
            pltpu.VMEM((width, group * HEAD_DIM), jnp.bfloat16),
            pltpu.VMEM((2, positions, 2 * HEAD_DIM), jnp.bfloat16),
            pltpu.VMEM((16, positions, 2 * HEAD_DIM), jnp.bfloat16),
            pltpu.VMEM((group, count, HEAD_DIM), jnp.bfloat16),
            pltpu.VMEM((group, count, HEAD_DIM), jnp.float32),
            pltpu.VMEM((group, count, 128), jnp.float32),
            pltpu.VMEM((group, count, 128), jnp.float32),
            pltpu.VMEM((2, 2, 2, 2, share, width), jnp.bfloat16),
            pltpu.VMEM((2, 2, 2, share, width), jnp.bfloat16),
            pltpu.VMEM((2, 2, 2, 2, share, width), jnp.bfloat16),
            pltpu.VMEM((2, 2, 2, share, width), jnp.bfloat16),
            pltpu.VMEM((2, 2, share, width), jnp.bfloat16),
            pltpu.VMEM((2, share, width), jnp.bfloat16),
            pltpu.VMEM(part, jnp.float32),
            pltpu.SemaphoreType.DMA((copies,)),
            pltpu.SemaphoreType.DMA((copies,)),
            pltpu.SemaphoreType.DMA((10,)),
        ],
        compiler_params=pltpu.CompilerParams(
            collective_id=0, has_side_effects=True, vmem_limit_bytes=63 * MIB
        ),
    )(
        source,
        target,
        key_w,
        value_w,
        query_w,
        out_w,
        source_gain,
        target_gain,
        final_gain.reshape(1, width),
        head_temp,
    )


def shifted(block, shift):
    size = lax.axis_size("tp")
    return lax.ppermute(block, "tp", [(i, (i + shift) % size) for i in range(size)])


def gather_rows(block):
    size = lax.axis_size("tp")
    return jnp.concatenate([block] + [shifted(block, k) for k in range(1, size)], axis=0)


def return_rows(blocks):
    size = lax.axis_size("tp")
    count = blocks.shape[0] // size
    mixed = blocks[:count].astype(jnp.float32)
    for k in range(1, size):
        mixed += shifted(blocks[k * count : (k + 1) * count], -k).astype(jnp.float32)
    return mixed


def flash_kernel(rows, query_ref, source_ref, mix_ref, total_ref, top_ref, sum_ref):
    step = pl.program_id(0)
    count = query_ref.shape[0]

    @pl.when(step == 0)
    def _():
        total_ref[...] = jnp.zeros_like(total_ref)
        sum_ref[...] = jnp.zeros_like(sum_ref)
        top_ref[...] = jnp.full_like(top_ref, FLOOR)

    for start in range(0, count, rows):
        block = pl.ds(start, rows)
        scores = lax.dot_general(
            query_ref[block, :],
            source_ref[...],
            (((1,), (1,)), ((), ())),
            preferred_element_type=jnp.float32,
        )
        old_top = top_ref[block, :1]
        new_top = jnp.maximum(old_top, jnp.max(scores, axis=-1, keepdims=True))
        shrink = jnp.exp2(old_top - new_top)
        expo = jnp.exp2(scores - new_top)
        top_ref[block, :] = jnp.broadcast_to(new_top, (rows, top_ref.shape[1]))
        new_sum = sum_ref[block, :1] * shrink + jnp.sum(expo, axis=-1, keepdims=True)
        sum_ref[block, :] = jnp.broadcast_to(new_sum, (rows, sum_ref.shape[1]))
        total_ref[block, :] = total_ref[block, :] * shrink + jnp.dot(
            expo.astype(jnp.bfloat16), source_ref[...], preferred_element_type=jnp.float32
        )

    @pl.when(step == pl.num_programs(0) - 1)
    def _():
        for start in range(0, count, rows):
            block = pl.ds(start, rows)
            mix_ref[block, :] = (total_ref[block, :] / sum_ref[block, :1]).astype(mix_ref.dtype)


def attend(query, source, chunk=CHUNK, rows=ROWS):
    count, width = query.shape
    positions = source.shape[0]
    chunk = math.gcd(chunk, positions)
    rows = math.gcd(rows, count)
    return pl.pallas_call(
        functools.partial(flash_kernel, rows),
        grid=(positions // chunk,),
        out_shape=jax.ShapeDtypeStruct((count, width), jnp.bfloat16),
        in_specs=[
            pl.BlockSpec((count, width), lambda j: (0, 0), pipeline_mode=pl.Buffered(1)),
            pl.BlockSpec((chunk, width), lambda j: (j, 0)),
        ],
        out_specs=pl.BlockSpec((count, width), lambda j: (0, 0), pipeline_mode=pl.Buffered(1)),
        scratch_shapes=[
            pltpu.VMEM((count, width), jnp.float32),
            pltpu.VMEM((count, 128), jnp.float32),
            pltpu.VMEM((count, 128), jnp.float32),
        ],
        compiler_params=pltpu.CompilerParams(
            dimension_semantics=("arbitrary",), vmem_limit_bytes=56 * 1024 * 1024
        ),
        cost_estimate=pl.CostEstimate(
            flops=4 * count * positions * width,
            bytes_accessed=2 * positions * width,
            transcendentals=count * positions,
        ),
    )(query, source)


def per_device(
    target, source, target_gain, source_gain, query_w, key_w, value_w, out_w, head_temp, final_gain
):
    width = target.shape[1]
    heads = query_w.shape[2] // HEAD_DIM
    shared = key_w.shape[2] // HEAD_DIM
    group = heads // shared
    positions = lax.all_gather(
        unit_rows(source).astype(jnp.bfloat16), ("sp", "tp"), axis=0, tiled=True
    )
    hidden_state = target.astype(jnp.float32)
    for layer in range(2):
        gain = source_gain[layer].astype(jnp.float32)
        normed = (unit_rows(hidden_state) * target_gain[layer].astype(jnp.float32)).astype(
            jnp.bfloat16
        )
        queries = jnp.dot(
            gather_rows(normed),
            query_w[layer],
            preferred_element_type=jnp.float32,
        ).astype(jnp.bfloat16)
        count = queries.shape[0]
        scales = head_temp[layer] * (HEAD_DIM ** (-0.5) * LOG2E)
        lifted = []
        for head in range(heads):
            columns = slice((head // group) * HEAD_DIM, (head // group + 1) * HEAD_DIM)
            lifted.append(
                (
                    lax.dot_general(
                        queries[:, head * HEAD_DIM : (head + 1) * HEAD_DIM],
                        key_w[layer][:, columns],
                        (((1,), (1,)), ((), ())),
                        preferred_element_type=jnp.float32,
                    )
                    * (gain * scales[head])
                ).astype(jnp.bfloat16)
            )
        mix = attend(jnp.concatenate(lifted, axis=0), positions)
        attended = []
        for head in range(heads):
            columns = slice((head // group) * HEAD_DIM, (head // group + 1) * HEAD_DIM)
            own = (mix[head * count : (head + 1) * count].astype(jnp.float32) * gain).astype(
                jnp.bfloat16
            )
            attended.append(
                jnp.dot(
                    own, value_w[layer][:, columns], preferred_element_type=jnp.float32
                ).astype(jnp.bfloat16)
            )
        mixed = return_rows(
            jnp.dot(
                jnp.concatenate(attended, axis=1),
                out_w[layer],
                preferred_element_type=jnp.float32,
            ).astype(jnp.bfloat16)
        )
        hidden_state = hidden_state + mixed
    return unit_rows(hidden_state) * final_gain.astype(jnp.float32)


def fits(mesh):
    return dict(mesh.shape) == {"sp": 8, "tp": 4}


def solution(mesh):
    in_specs = (
        P(("sp", "tp"), None),
        P(("sp", "tp"), None),
        P(),
        P(),
        P(None, None, "tp"),
        P(None, None, "tp"),
        P(None, None, "tp"),
        P(None, "tp", None),
        P(None, "tp"),
        P(),
    )
    out_specs = P(("sp", "tp"), None)
    return jax.shard_map(
        on_planes if fits(mesh) else per_device, mesh=mesh, in_specs=in_specs, out_specs=out_specs, check_vma=False
    )
```
